32 devices in a mesh: fs: 4 (over z), rep: 4 (over y, x), tp: 2 (over core).
Axes of the slice: x: 2, y: 2, z: 4, core: 2. Of those that a mesh axis runs over, the one named last changes fastest.
Arguments:
- mixer_input: bfloat16 [32768, 2048], P(('fs', 'rep')), may hold values from -6 to 6
- value_cot: bfloat16 [32768, 2048], P(('fs', 'rep'), 'tp'), may hold values from -0.22097087 to 0.22097087
- gate_cot: bfloat16 [32768, 2048], P(('fs', 'rep'), 'tp'), may hold values from -0.22097087 to 0.22097087
- value_weight: float32 [2048, 2048], P('fs', 'tp'), may hold values from -0.125 to 0.125
- gate_weight: float32 [2048, 2048], P('fs', 'tp'), may hold values from -0.125 to 0.125
- value_basis: bfloat16 [2048, 256], replicated, may hold values from -0.8838835 to 0.8838835
- gate_basis: bfloat16 [2048, 256], replicated, may hold values from -0.8838835 to 0.8838835
- value_first: float32 [256, 2048], P('fs', 'tp'), may hold values from -6 to 6
- gate_first: float32 [256, 2048], P('fs', 'tp'), may hold values from -6 to 6
- value_second: float32 [256, 2048], P('fs', 'tp'), may hold values from 0.01 to 1
- gate_second: float32 [256, 2048], P('fs', 'tp'), may hold values from 0.01 to 1
Outputs:
- value_new: float32 [2048, 2048], P('fs', 'tp')
- gate_new: float32 [2048, 2048], P('fs', 'tp')
- value_copy: bfloat16 [2048, 2048], P(None, 'tp')
- gate_copy: bfloat16 [2048, 2048], P(None, 'tp')
- value_step: float32 [2048, 2048], P('fs', 'tp')
- gate_step: float32 [2048, 2048], P('fs', 'tp')
- value_first_new: float32 [256, 2048], P('fs', 'tp')
- gate_first_new: float32 [256, 2048], P('fs', 'tp')
- value_second_new: float32 [256, 2048], P('fs', 'tp')
- gate_second_new: float32 [256, 2048], P('fs', 'tp')
The draws below stay inside these ranges and needn't reach their ends.
All inputs are finite; a program needn't handle non-finite values.
Results may differ from the reference program's by a relative error of at most 0.0044.
Values may be sent and summed in bfloat16 or wider, within the bound.
A program may use at most 128 MiB of HBM per device.

```python
import math
import jax
import jax.numpy as jnp
from jax import lax

D = 2048
R = 256
TOKENS = 32768


def cot_helper(key, salt):
    key = jax.random.fold_in(key, salt)
    first_key, second_key = jax.random.split(key, 2)
    base = jnp.clip(jax.random.normal(first_key, (TOKENS, D), jnp.float32), -6.0, 6.0)
    ramp = jnp.exp(jnp.log(3.0) * jnp.arange(D, dtype=jnp.float32) / (D - 1))
    jitter = jnp.exp(jax.random.uniform(second_key, (D,), jnp.float32) * jnp.log(2.0))
    limit = 40.0 * TOKENS ** (-0.5)
    values = base * (ramp * jitter)[None, :] * TOKENS ** (-0.5)
    return jnp.clip(values, -limit, limit)


def basis_helper(key, salt):
    key = jax.random.fold_in(key, salt)
    first_key, second_key = jax.random.split(key, 2)
    base = jnp.clip(jax.random.normal(first_key, (D, R), jnp.float32), -6.0, 6.0)
    top = 4.0
    ramp = jnp.exp(jnp.log(top) * jnp.arange(D, dtype=jnp.float32) / (D - 1))
    jitter = jnp.exp(jax.random.uniform(second_key, (D,), jnp.float32) * jnp.log(2.0))
    limit = 40.0 * D ** (-0.5)
    values = base * (ramp * jitter)[:, None] * D ** (-0.5)
    return jnp.clip(values, -limit, limit)


def draw_value_cot(key, part):
    return cot_helper(key, 11).astype(jnp.bfloat16)


def draw_gate_cot(key, part):
    return cot_helper(key, 23).astype(jnp.bfloat16)


def draw_value_basis(key, part):
    return basis_helper(key, 37).astype(jnp.bfloat16)


def draw_gate_basis(key, part):
    return basis_helper(key, 41).astype(jnp.bfloat16)


def block_scale(key, shape, shards, least, largest):
    def one(position, parts):
        steps = jax.random.uniform(jax.random.fold_in(jax.random.fold_in(key, 6), position), (parts,), jnp.float32, least / len(shards), largest / len(shards))
        return jnp.repeat(jnp.exp(steps), shape[position] // parts).reshape((-1,) + (1,) * (len(shape) - position - 1))

    level = one(*shards[0])
    for cut in shards[1:]:
        level = level * one(*cut)
    return level


def normal_values(key, extent, deviation, reach, cuts=(), kind=jnp.bfloat16):
    loudness = block_scale(key, extent, cuts, -0.22, 0.18) if cuts else 1.0
    array = jax.random.normal(key, extent, jnp.float32) * deviation * loudness
    return jnp.minimum(jnp.maximum(array, -reach), reach).astype(kind)


def setup_inputs(seed: int = 0) -> dict:
    streams_of = jax.random.split(jax.random.key(seed), 12)
    mixer_input = normal_values(streams_of[0], (TOKENS, D), 1.0, 6.0, ((0, 16),))
    value_cot = draw_value_cot(jax.random.fold_in(streams_of[11], 71), 0)
    gate_cot = draw_gate_cot(jax.random.fold_in(streams_of[11], 71), 0)
    value_weight = normal_values(streams_of[3], (D, D), D ** -0.5, 0.125, ((0, 4), (1, 2)), jnp.float32)
    gate_weight = normal_values(streams_of[4], (D, D), D ** -0.5, 0.125, ((0, 4), (1, 2)), jnp.float32)
    value_basis = draw_value_basis(jax.random.fold_in(streams_of[11], 71), 0)
    gate_basis = draw_gate_basis(jax.random.fold_in(streams_of[11], 71), 0)
    value_first = normal_values(streams_of[7], (R, D), 1.0, 6.0, ((0, 4), (1, 2)), jnp.float32)
    gate_first = normal_values(streams_of[8], (R, D), 1.0, 6.0, ((0, 4), (1, 2)), jnp.float32)
    value_second = jnp.clip(jnp.exp(math.log(1.0) - 4.6051702 * jax.random.uniform(streams_of[9], (R, D), jnp.float32) ** block_scale(streams_of[9], (R, D), ((0, 4), (1, 2)), -0.2, 0.2)), 0.01, 1.0)
    gate_second = jnp.clip(jnp.exp(math.log(1.0) - 4.6051702 * jax.random.uniform(streams_of[10], (R, D), jnp.float32) ** block_scale(streams_of[10], (R, D), ((0, 4), (1, 2)), -0.2, 0.2)), 0.01, 1.0)
    return {"mixer_input": mixer_input, "value_cot": value_cot, "gate_cot": gate_cot, "value_weight": value_weight, "gate_weight": gate_weight, "value_basis": value_basis, "gate_basis": gate_basis, "value_first": value_first, "gate_first": gate_first, "value_second": value_second, "gate_second": gate_second}


learn_rate = 0.02

def one_role(mixer_input, cotangent, weight, basis, first, second):
    gradient = jnp.dot(mixer_input.T, cotangent, preferred_element_type=jnp.float32)
    projected = jnp.dot(basis.astype(jnp.float32).T, gradient, precision=lax.Precision.HIGHEST)
    first_new = 0.9 * first + 0.1 * projected
    second_new = 0.95 * second + 0.05 * projected * projected
    scaled = (first_new * lax.rsqrt(second_new)).astype(jnp.bfloat16)
    expanded = jnp.dot(basis, scaled, preferred_element_type=jnp.float32)
    direction = expanded * lax.rsqrt(jnp.mean(expanded * expanded) + 1e-06)
    updated = weight - learn_rate * direction
    return (updated, updated.astype(jnp.bfloat16), direction, first_new, second_new)

def reference(mixer_input, value_cot, gate_cot, value_weight, gate_weight, value_basis, gate_basis, value_first, gate_first, value_second, gate_second):
    v_out = one_role(mixer_input, value_cot, value_weight, value_basis, value_first, value_second)
    g_out = one_role(mixer_input, gate_cot, gate_weight, gate_basis, gate_first, gate_second)
    return (v_out[0], g_out[0], v_out[1], g_out[1], v_out[2], g_out[2], v_out[3], g_out[3], v_out[4], g_out[4])
```

```python
import functools

import jax
import jax.numpy as jnp
from jax import lax
from jax.experimental import pallas as pl
from jax.experimental.pallas import tpu as pltpu
from jax.sharding import PartitionSpec as P

learn_rate = 0.02
CHUNKS = 4
VMEM_FIRST = 40 * 1024 * 1024
VMEM_SECOND = 40 * 1024 * 1024
F32 = jnp.float32
BF16 = jnp.bfloat16


def dot(a, b):
    return jnp.dot(a, b, preferred_element_type=F32)


def dot_first(a, b):
    return lax.dot_general(a, b, (((0,), (0,)), ((), ())), preferred_element_type=F32)


def split(a):
    upper = a.astype(BF16)
    return upper, (a - upper.astype(F32)).astype(BF16)


def exchange(
    n_fs, n_rep, n_tp,
    mixer, value_cot, gate_cot, value_weight, gate_weight, value_basis, gate_basis,
    value_first_hbm, gate_first_hbm, value_second_hbm, gate_second_hbm,
    value_rows, gate_rows, scaled_out, projected_out, squares_out,
    x_buf, cot_buf, w_buf, w_half, basis_buf, gram, acc, part_in,
    mid, mid_in, proj_all, scaled, sq_buf, moments,
    x_sem, w_sem, b_sem, own_sem, m_sem,
    w1_send, w1_recv, w2_send, w2_recv,
    s1_send, s1_recv, s2_send, s2_recv, p_send, p_recv, a_send, a_recv, g_send, g_recv, q_send, q_recv,
):
    f, r, t = lax.axis_index("fs"), lax.axis_index("rep"), lax.axis_index("tp")
    cots = (value_cot, gate_cot)
    weights = (value_weight, gate_weight)
    bases = (value_basis, gate_basis)
    gathered = (value_rows, gate_rows)
    tokens = mixer.shape[0]
    chunk = tokens // CHUNKS
    rows = value_weight.shape[0]
    share = rows // n_rep
    width = acc.shape[2]
    per_role = n_rep // 2
    low = mid.shape[1]

    def fs_at(d):
        return lax.rem(f + d, n_fs)

    def rep_at(d):
        return lax.rem(r + d, n_rep)

    def send(src, dst, s, v, **where):
        return pltpu.make_async_remote_copy(
            src_ref=src, dst_ref=dst, send_sem=s, recv_sem=v,
            device_id=where, device_id_type=pl.DeviceIdType.MESH,
        )

    w_loads = [pltpu.make_async_copy(weights[k], w_buf.at[k], w_sem.at[k]) for k in range(2)]
    b_loads = [pltpu.make_async_copy(bases[k], basis_buf.at[k], b_sem.at[k]) for k in range(2)]

    def x_loads(c):
        span = pl.ds(pl.multiple_of(c * chunk, chunk), chunk)
        return [pltpu.make_async_copy(mixer.at[span], x_buf.at[c], x_sem.at[c, 0])] + [
            pltpu.make_async_copy(cots[k].at[span], cot_buf.at[k, c], x_sem.at[c, 1 + k]) for k in range(2)
        ]

    m_loads = [
        pltpu.make_async_copy(ref, moments.at[i], m_sem.at[i])
        for i, ref in enumerate((value_first_hbm, gate_first_hbm, value_second_hbm, gate_second_hbm))
    ]
    for copy in w_loads + b_loads:
        copy.start()
    for c in range(CHUNKS):
        for copy in x_loads(c):
            copy.start()

    for copy in m_loads:
        copy.start()

    barrier = pltpu.get_barrier_semaphore()
    for d in range(1, n_fs):
        pl.semaphore_signal(barrier, inc=1, device_id={"fs": fs_at(d)}, device_id_type=pl.DeviceIdType.MESH)
    for d in range(1, n_rep):
        pl.semaphore_signal(barrier, inc=1, device_id={"rep": rep_at(d)}, device_id_type=pl.DeviceIdType.MESH)
    for d in range(1, n_tp):
        pl.semaphore_signal(
            barrier, inc=1, device_id={"tp": lax.rem(t + d, n_tp)}, device_id_type=pl.DeviceIdType.MESH
        )
    for k in range(2):
        w_loads[k].wait()
        w_half[k] = w_buf[k].astype(BF16)
    pl.semaphore_wait(barrier, n_fs + n_rep + n_tp - 3)

    def share_of(block, part_index):
        return pl.ds(pl.multiple_of(block * rows + part_index * share, share), share)

    w1 = {}
    for d in range(1, n_fs):
        for k in range(2):
            w1[d, k] = send(
                w_half.at[k, pl.ds(pl.multiple_of(r * share, share), share)],
                gathered[k].at[share_of(f, r)],
                w1_send.at[d - 1, k], w1_recv.at[d - 1, k], fs=fs_at(d),
            )
            w1[d, k].start()
    own = []
    for k in range(2):
        copy = pltpu.make_async_copy(
            w_half.at[k], gathered[k].at[pl.ds(pl.multiple_of(f * rows, rows), rows)], own_sem.at[k]
        )
        copy.start()
        own.append(copy)

    for copy in b_loads:
        copy.wait()
    acc[...] = jnp.zeros_like(acc)

    def one_chunk(c, carry):
        for copy in x_loads(c):
            copy.wait()
        x = x_buf[c]
        for k in range(2):
            upper, lower = split(dot(x, basis_buf[k]))
            for q in range(per_role):
                cols = slice(q * width, (q + 1) * width)
                cot = cot_buf[k, c, :, cols]
                acc[k * per_role + q] += dot_first(upper, cot) + dot_first(lower, cot)
        return carry

    lax.fori_loop(0, CHUNKS, one_chunk, 0)
    s1 = {}
    for d in range(1, n_rep):
        s1[d] = send(
            acc.at[rep_at(d)], part_in.at[d - 1], s1_send.at[d - 1], s1_recv.at[d - 1], rep=rep_at(d)
        )
        s1[d].start()

    w2, heard = {}, set()
    near, far = (r + 1 - 2 * lax.rem(r, 2), lax.rem(r + 2, n_rep)) if n_rep == 4 else (None, None)

    def pass_on(d, e, k, owner, peer):
        source = lax.rem(f - d + n_fs, n_fs)
        rows_ref = gathered[k].at[share_of(source, owner)]
        w2[d, e, k] = send(
            rows_ref, rows_ref, w2_send.at[d - 1, e, k], w2_recv.at[d - 1, e, k], rep=peer
        )
        w2[d, e, k].start()

    def forward(d):
        for k in range(2):
            w1[d, k].wait_recv()
            peers = (near, far) if n_rep == 4 else [rep_at(e) for e in range(1, n_rep)]
            for e, peer in enumerate(peers):
                pass_on(d, e, k, r, peer)

    def relay(d):
        if n_rep == 4:
            for e, k, owner, peer in ((0, 0, near, far), (1, 1, far, near)):
                w2[d, e, k].wait_recv()
                heard.add((d, e, k))
                pass_on(d, 2, k, owner, peer)

    forward(1)
    for k in range(2):
        upper, lower = split(dot_first(basis_buf[k], basis_buf[k]))
        gram[k, 0] = upper
        gram[k, 1] = lower

    for d in range(1, n_rep):
        s1[d].wait_recv()
    total = acc[r]
    for d in range(1, n_rep):
        total += part_in[d - 1]
    mid[...] = total.reshape(mid.shape)
    s2 = {}
    for d in range(1, n_fs):
        s2[d] = send(
            mid.at[fs_at(d)], mid_in.at[d - 1], s2_send.at[d - 1], s2_recv.at[d - 1], fs=fs_at(d)
        )
        s2[d].start()
    for d in range(2, n_fs - 1):
        forward(d)
        relay(d - 1)
    for d in range(1, n_fs):
        s2[d].wait_recv()
    small = mid[f]
    for d in range(1, n_fs):
        small += mid_in[d - 1]
    proj_all[r] = small.astype(BF16)

    cols = pl.ds(pl.multiple_of(lax.rem(r, per_role) * width, width), width)
    is_value = r < per_role
    for copy in m_loads:
        copy.wait()
    first = jnp.where(is_value, moments[0, :, cols], moments[1, :, cols])
    second = jnp.where(is_value, moments[2, :, cols], moments[3, :, cols])
    first_new = 0.9 * first + 0.1 * small
    second_new = 0.95 * second + 0.05 * small * small
    scaled[r, f] = (first_new * lax.rsqrt(second_new)).astype(BF16)
    a4, p4, g4 = {}, {}, {}
    for d in range(1, n_fs):
        a4[d] = send(
            scaled.at[r, f], scaled.at[r, f], a_send.at[d - 1], a_recv.at[d - 1], fs=fs_at(d)
        )
        a4[d].start()
    for d in range(1, n_rep):
        p4[d] = send(proj_all.at[r], proj_all.at[r], p_send.at[d - 1], p_recv.at[d - 1], rep=rep_at(d))
        p4[d].start()
    if n_fs > 2:
        forward(n_fs - 1)
        relay(n_fs - 2)
    for d in range(1, n_fs):
        a4[d].wait_recv()
    for d in range(1, n_rep):
        g4[d] = send(scaled.at[r], scaled.at[r], g_send.at[d - 1], g_recv.at[d - 1], rep=rep_at(d))
        g4[d].start()
    relay(n_fs - 1)
    for d in range(1, n_rep):
        g4[d].wait_recv()

    for k in range(2):
        squares = 0.0
        for q in range(per_role):
            s = scaled[k * per_role + q].reshape(n_fs * low, width)
            squares += jnp.sum((dot(gram[k, 0], s) + dot(gram[k, 1], s)) * s.astype(F32))
        sq_buf[0, k] = jnp.full(sq_buf.shape[2:], squares, F32)
    q4 = []
    for d in range(1, n_tp):
        copy = send(
            sq_buf.at[0], sq_buf.at[d], q_send.at[d - 1], q_recv.at[d - 1], tp=lax.rem(t + d, n_tp)
        )
        copy.start()
        q4.append(copy)
    for d in range(1, n_rep):
        p4[d].wait_recv()
    scaled_out[...] = scaled[...].reshape(scaled_out.shape)
    projected_out[...] = proj_all[...]
    for copy in q4:
        copy.wait_recv()
    sums = sq_buf[0]
    for d in range(1, n_tp):
        sums += sq_buf[d]
    squares_out[...] = sums

    for copy in list(w1.values()) + list(s1.values()) + list(s2.values()) + list(a4.values()):
        copy.wait_send()
    for copy in list(p4.values()) + list(g4.values()) + q4:
        copy.wait_send()
    for copy in own:
        copy.wait()
    for key, copy in w2.items():
        copy.wait_send()
        if key not in heard:
            copy.wait_recv()


def finish(
    own_blocks, entries,
    where, value_rows, gate_rows, value_basis, gate_basis, value_weight, gate_weight,
    scaled, projected, squares, value_first, gate_first, value_second, gate_second,
    value_new, gate_new, value_copy, gate_copy, value_step, gate_step,
    value_first_new, gate_first_new, value_second_new, gate_second_new,
):
    step = pl.program_id(0)
    width = scaled.shape[2]
    per_role = scaled.shape[0] // 2
    roles = (
        (value_rows, value_basis, value_weight, value_new, value_copy, value_step),
        (gate_rows, gate_basis, gate_weight, gate_new, gate_copy, gate_step),
    )
    for k, (rows, basis, weight, new, copy, step_out) in enumerate(roles):
        factor = lax.rsqrt(squares[k, :1, :1] / entries + 1e-06)
        for q in range(per_role):
            cols = slice(q * width, (q + 1) * width)
            direction = dot(basis[...], scaled[k * per_role + q]) * factor
            copy[:, cols] = (rows[:, cols].astype(F32) - learn_rate * direction).astype(BF16)

            @pl.when(step < own_blocks)
            def _():
                step_out[:, cols] = direction
                new[:, cols] = weight[:, cols] - learn_rate * direction

    @pl.when(step == 0)
    def _():
        moments = (
            (value_first, value_second, value_first_new, value_second_new),
            (gate_first, gate_second, gate_first_new, gate_second_new),
        )
        for k, (first, second, first_new, second_new) in enumerate(moments):
            for q in range(per_role):
                cols = slice(q * width, (q + 1) * width)
                small = projected[k * per_role + q].astype(F32)
                first_new[:, cols] = 0.9 * first[:, cols] + 0.1 * small
                second_new[:, cols] = 0.95 * second[:, cols] + 0.05 * small * small


def local(sizes, *args):
    n_fs, n_rep, n_tp = sizes
    (mixer, value_cot, gate_cot, value_weight, gate_weight, value_basis, gate_basis,
     value_first, gate_first, value_second, gate_second) = args
    tokens, model = mixer.shape
    half = value_cot.shape[1]
    rows = value_weight.shape[0]
    rank = value_basis.shape[1]
    low = value_first.shape[0]
    width = 2 * half // n_rep
    chunk = tokens // CHUNKS
    any_spec = pl.BlockSpec(memory_space=pl.ANY)
    vmem = pl.BlockSpec(memory_space=pltpu.VMEM)
    dma = pltpu.SemaphoreType.DMA
    scratch = [
        pltpu.VMEM((CHUNKS, chunk, model), BF16),
        pltpu.VMEM((2, CHUNKS, chunk, half), BF16),
        pltpu.VMEM((2, rows, half), F32),
        pltpu.VMEM((2, rows, half), BF16),
        pltpu.VMEM((2, model, rank), BF16),
        pltpu.VMEM((2, 2, rank, rank), BF16),
        pltpu.VMEM((n_rep, rank, width), F32),
        pltpu.VMEM((n_rep - 1, rank, width), F32),
        pltpu.VMEM((n_fs, low, width), F32),
        pltpu.VMEM((n_fs - 1, low, width), F32),
        pltpu.VMEM((n_rep, low, width), BF16),
        pltpu.VMEM((n_rep, n_fs, low, width), BF16),
        pltpu.VMEM((n_tp, 2, 8, 128), F32),
        pltpu.VMEM((4, low, half), F32),
        dma((CHUNKS, 3)), dma((2,)), dma((2,)), dma((2,)), dma((4,)),
        dma((n_fs - 1, 2)), dma((n_fs - 1, 2)),
        dma((n_fs - 1, n_rep - 1, 2)), dma((n_fs - 1, n_rep - 1, 2)),
    ]
    for count in (n_rep, n_fs, n_rep, n_fs, n_rep, n_tp):
        scratch += [dma((count - 1,)), dma((count - 1,))]
    value_rows, gate_rows, scaled, projected, squares = pl.pallas_call(
        functools.partial(exchange, n_fs, n_rep, n_tp),
        out_shape=(
            jax.ShapeDtypeStruct((rows * n_fs, half), BF16),
            jax.ShapeDtypeStruct((rows * n_fs, half), BF16),
            jax.ShapeDtypeStruct((n_rep, rank, width), BF16),
            jax.ShapeDtypeStruct((n_rep, low, width), BF16),
            jax.ShapeDtypeStruct((2, 8, 128), F32),
        ),
        in_specs=[any_spec] * 11,
        out_specs=(any_spec, any_spec, vmem, vmem, vmem),
        scratch_shapes=scratch,
        compiler_params=pltpu.CompilerParams(
            collective_id=0, has_side_effects=True, vmem_limit_bytes=52 * 1024 * 1024
        ),
        name="exchange",
    )(*args)

    block = min(rows, 256)
    own_blocks = rows // block
    blocks = model // block
    where = (lax.axis_index("fs") * own_blocks).astype(jnp.int32).reshape(1)

    def turned(i, w):
        return (lax.rem(w[0] + i, blocks), 0)

    def own(i, w):
        return (jnp.minimum(i, own_blocks - 1), 0)

    def whole(shape):
        return pl.BlockSpec(shape, lambda i, w: (0,) * len(shape))

    row_spec = pl.BlockSpec((block, half), turned)
    basis_spec = pl.BlockSpec((block, rank), turned)
    own_spec = pl.BlockSpec((block, half), own)
    moment = whole((low, half))
    return pl.pallas_call(
        functools.partial(finish, own_blocks, float(model) * half * n_tp),
        grid_spec=pltpu.PrefetchScalarGridSpec(
            num_scalar_prefetch=1,
            grid=(blocks,),
            in_specs=[row_spec, row_spec, basis_spec, basis_spec, own_spec, own_spec,
                      whole(scaled.shape), whole(projected.shape), whole(squares.shape)] + [moment] * 4,
            out_specs=[own_spec, own_spec, row_spec, row_spec, own_spec, own_spec] + [moment] * 4,
        ),
        out_shape=[
            jax.ShapeDtypeStruct((rows, half), F32),
            jax.ShapeDtypeStruct((rows, half), F32),
            jax.ShapeDtypeStruct((model, half), BF16),
            jax.ShapeDtypeStruct((model, half), BF16),
            jax.ShapeDtypeStruct((rows, half), F32),
            jax.ShapeDtypeStruct((rows, half), F32),
        ] + [jax.ShapeDtypeStruct((low, half), F32)] * 4,
        compiler_params=pltpu.CompilerParams(vmem_limit_bytes=40 * 1024 * 1024),
        name="finish",
    )(where, value_rows, gate_rows, value_basis, gate_basis, value_weight, gate_weight,
      scaled, projected, squares, value_first, gate_first, value_second, gate_second)


EXTRA = ()
RELAY_X = (0, 1)
RELAY_Y = (2, 3)


def exchange_block(
    mixer, value_cot, gate_cot, value_weight, gate_weight, value_basis, gate_basis,
    value_first, gate_first, value_second, gate_second,
    gathered, scaled, proj, squares_out, basis, weight, moments,
    x_buf, cot_buf, gram, acc, first_in, second_out, second_in, part, part_in, sq_buf,
    x_sem, c_sem, b_sem, w_sem, m_sem,
    z_send, z_recv, x_send, x_recv, y_send, y_recv, rx_send, rx_recv, ry_send, ry_recv,
    s1_send, s1_recv, s2_send, s2_recv, s3_send, s3_recv, a_send, a_recv,
    g_send, g_recv, p_send, p_recv, q_send, q_recv,
):
    f, r, t = lax.axis_index("fs"), lax.axis_index("rep"), lax.axis_index("tp")
    n_fs = 4
    cots = (value_cot, gate_cot)
    weights = (value_weight, gate_weight)
    bases = (value_basis, gate_basis)
    tokens = mixer.shape[0]
    chunk = tokens // CHUNKS
    rows = value_weight.shape[0]
    share = rows // 4
    piece_rows = share // 2
    low = moments.shape[1]
    width = acc.shape[3]
    ends = jnp.logical_or(f == 0, f == n_fs - 1)
    inner = jnp.logical_not(ends)
    turn = 1 - 2 * (f // 2)
    ahead = f + turn
    behind = jnp.clip(f - turn, 0, n_fs - 1)
    x_at, y_at = lax.rem(r, 2), r // 2
    x_peer, y_peer = r + 1 - 2 * x_at, r + 2 - 4 * y_at
    across = 3 - r
    half_at, part_at = (x_at, y_at), (y_at, x_at)
    half_peer, part_peer = (x_peer, y_peer), (y_peer, x_peer)
    mine = [2 * half_at[k] + part_at[k] for k in range(2)]

    def fs_at(d):
        return lax.rem(f + d, n_fs)

    def send(src, dst, s, v, **where):
        return pltpu.make_async_remote_copy(
            src_ref=src, dst_ref=dst, send_sem=s, recv_sem=v,
            device_id=where, device_id_type=pl.DeviceIdType.MESH,
        )

    def span(start, size):
        return pl.ds(pl.multiple_of(start, size), size)

    def piece(plane, quarter, c):
        return gathered.at[c % 2, span(plane * rows + quarter * share + (c // 2) * piece_rows, piece_rows)]

    z_pieces = [(r, c) for c in range(4)] + [(across, c) for c in EXTRA]
    count = len(z_pieces)
    order = (r, across, x_peer, y_peer)

    def w_load(o, k):
        where = span(order[o] * share, share)
        return pltpu.make_async_copy(weights[k].at[where], weight.at[k, where], w_sem.at[o, k])

    def b_load(k):
        return pltpu.make_async_copy(bases[k], basis.at[k], b_sem.at[k])

    def x_load(c):
        return pltpu.make_async_copy(mixer.at[span(c * chunk, chunk)], x_buf.at[c], x_sem.at[c])

    def c_load(k, c):
        return pltpu.make_async_copy(cots[k].at[span(c * chunk, chunk)], cot_buf.at[k, c], c_sem.at[k, c])

    m_loads = [
        pltpu.make_async_copy(ref, moments.at[i], m_sem.at[i])
        for i, ref in enumerate((value_first, gate_first, value_second, gate_second))
    ]
    for k in range(2):
        w_load(0, k).start()
    if EXTRA:
        for k in range(2):
            w_load(1, k).start()
    b_load(0).start()
    for c in range(CHUNKS):
        x_load(c).start()
        c_load(0, c).start()
    b_load(1).start()
    for c in range(CHUNKS):
        c_load(1, c).start()
    for copy in m_loads:
        copy.start()
    for o in range(2 if EXTRA else 1, 4):
        for k in range(2):
            w_load(o, k).start()

    barrier = pltpu.get_barrier_semaphore()
    for d in range(1, n_fs):
        pl.semaphore_signal(barrier, inc=1, device_id={"fs": fs_at(d)}, device_id_type=pl.DeviceIdType.MESH)
    for peer in (x_peer, y_peer):
        pl.semaphore_signal(barrier, inc=1, device_id={"rep": peer}, device_id_type=pl.DeviceIdType.MESH)
    pl.semaphore_signal(barrier, inc=1, device_id={"tp": 1 - t}, device_id_type=pl.DeviceIdType.MESH)

    for o in range(2 if EXTRA else 1):
        where = span(order[o] * share, share)
        for k in range(2):
            w_load(o, k).wait()
            gathered[k, span(f * rows + order[o] * share, share)] = weight[k, where].astype(BF16)
    pl.semaphore_wait(barrier, n_fs + 2)

    def plane_of(slot):
        return lax.rem(f + turn * slot + n_fs, n_fs)

    landing = jnp.where(ends, 2, 0)

    def own_ahead(i):
        quarter, c = z_pieces[i]
        ref = piece(f, quarter, c)
        return send(ref, ref, z_send.at[0, i], z_recv.at[landing, i], fs=ahead)

    def own_behind(i):
        quarter, c = z_pieces[i]
        ref = piece(f, quarter, c)
        return send(ref, ref, z_send.at[1, i], z_recv.at[0, i], fs=behind)

    def pass_along(slot, i):
        quarter, c = z_pieces[i]
        ref = piece(plane_of(slot), quarter, c)
        if slot == 3:
            return send(ref, ref, z_send.at[4, i], z_recv.at[1, i], fs=ahead)
        return send(ref, ref, z_send.at[1 + slot, i], z_recv.at[slot, i], fs=behind)

    def arrival(slot, i):
        quarter, c = z_pieces[i]
        ref = piece(plane_of(slot), quarter, c)
        return send(ref, ref, z_send.at[0, i], z_recv.at[slot - 1, i], fs=ahead)

    for i in range(count):
        own_ahead(i).start()

        @pl.when(inner)
        def _():
            own_behind(i).start()

    def to_x(slot, c):
        ref = piece(plane_of(slot), r, c)
        return send(ref, ref, x_send.at[slot - 1, c], x_recv.at[slot - 1, c], rep=x_peer)

    def to_y(slot, c):
        ref = piece(plane_of(slot), r, c)
        return send(ref, ref, y_send.at[slot - 1, c], y_recv.at[slot - 1, c], rep=y_peer)

    def relay_x(slot, c):
        ref = piece(plane_of(slot), y_peer, c)
        return send(ref, ref, rx_send.at[slot - 1, c], rx_recv.at[slot - 1, c], rep=x_peer)

    def relay_y(slot, c):
        ref = piece(plane_of(slot), x_peer, c)
        return send(ref, ref, ry_send.at[slot - 1, c], ry_recv.at[slot - 1, c], rep=y_peer)

    def spread(slot, i):
        if i < 4:
            to_x(slot, i).start()
            to_y(slot, i).start()

    def arrive_first(i):
        arrival(1, i).wait_recv()

        @pl.when(inner)
        def _():
            pass_along(1, i).start()

        spread(1, i)

    def arrive_inner(i):
        @pl.when(inner)
        def _():
            arrival(3, i).wait_recv()
            pass_along(3, i).start()

    def arrive_second(i):
        arrival(2, i).wait_recv()

        @pl.when(inner)
        def _():
            pass_along(2, i).start()

        spread(2, i)

    def arrive_third(i):
        @pl.when(ends)
        def _():
            arrival(3, i).wait_recv()

        spread(3, i)

    def relay(slot, c):
        if c in RELAY_X:
            to_y(slot, c).wait_recv()
            relay_x(slot, c).start()
        if c in RELAY_Y:
            to_x(slot, c).wait_recv()
            relay_y(slot, c).start()

    def s1(k):
        other = acc.at[k, pl.ds(2 * (1 - half_at[k]), 2)]
        return send(other, first_in.at[k], s1_send.at[k], s1_recv.at[k], rep=half_peer[k])

    def s2(k):
        return send(second_out.at[k], second_in.at[k], s2_send.at[k], s2_recv.at[k], rep=part_peer[k])

    def s3(k, d):
        return send(
            part.at[k, span(fs_at(d) * low, low)], part_in.at[k, d - 1],
            s3_send.at[k, d - 1], s3_recv.at[k, d - 1], fs=fs_at(d),
        )

    def halve(k):
        s1(k).wait_recv()
        other = 1 - part_at[k]
        second_out[k] = acc[k, 2 * half_at[k] + other] + first_in[k, other]
        s2(k).start()
        part[k] = acc[k, mine[k]] + first_in[k, part_at[k]]

    def quarter(k):
        s2(k).wait_recv()
        part[k] += second_in[k]
        for d in range(1, n_fs):
            s3(k, d).start()

    def a4(k, d):
        ref = scaled.at[k, mine[k], span(f * low, low)]
        return send(ref, ref, a_send.at[k, d - 1], a_recv.at[k, d - 1], fs=fs_at(d))

    def grow(buf, ss, vs, k, stage):
        if stage == 0:
            ref = buf.at[k, mine[k]]
            return send(ref, ref, ss.at[k, 0], vs.at[k, 0], rep=part_peer[k])
        if stage == 1:
            ref = buf.at[k, mine[k]]
            return send(ref, ref, ss.at[k, 1], vs.at[k, 1], rep=half_peer[k])
        ref = buf.at[k, 2 * half_at[k] + 1 - part_at[k]]
        return send(ref, ref, ss.at[k, 2], vs.at[k, 2], rep=half_peer[k])

    def g4(k, stage):
        return grow(scaled, g_send, g_recv, k, stage)

    def p4(k, stage):
        return grow(proj, p_send, p_recv, k, stage)

    def update(k):
        if k == 0:
            for copy in m_loads:
                copy.wait()
        for d in range(1, n_fs):
            s3(k, d).wait_recv()
        small = part[k, span(f * low, low)]
        for d in range(1, n_fs):
            small += part_in[k, d - 1]
        proj[k, mine[k]] = small
        cols = span(mine[k] * width, width)
        first_new = 0.9 * moments[k, :, cols] + 0.1 * small
        second_new = 0.95 * moments[2 + k, :, cols] + 0.05 * small * small
        scaled[k, mine[k], span(f * low, low)] = (first_new * lax.rsqrt(second_new)).astype(BF16)
        for d in range(1, n_fs):
            a4(k, d).start()

    def collect(k):
        for d in range(1, n_fs):
            a4(k, d).wait_recv()
        g4(k, 0).start()
        g4(k, 1).start()
        p4(k, 0).start()
        p4(k, 1).start()

    def collect_second(k):
        g4(k, 0).wait_recv()
        g4(k, 2).start()
        p4(k, 0).wait_recv()
        p4(k, 2).start()

    def measure(k):
        for stage in (1, 2):
            g4(k, stage).wait_recv()
        squares = 0.0
        for n in range(4):
            s = scaled[k, n]
            squares += jnp.sum((dot(gram[k, 0], s) + dot(gram[k, 1], s)) * s.astype(F32))
        sq_buf[0, k] = jnp.full(sq_buf.shape[2:], squares, F32)

    def make_gram():
        for k in range(2):
            upper, lower = split(dot_first(basis[k], basis[k]))
            gram[k, 0] = upper
            gram[k, 1] = lower

    acc[...] = jnp.zeros_like(acc)
    b_load(0).wait()

    def one_step(i, carry):
        k, c = i // CHUNKS, lax.rem(i, CHUNKS)

        @pl.when(k == 0)
        def _():
            x_load(c).wait()
            c_load(0, c).wait()

        @pl.when(k == 1)
        def _():
            c_load(1, c).wait()

        @pl.when(i == CHUNKS)
        def _():
            s1(0).start()
            b_load(1).wait()

        for at, job in ((CHUNKS + 1, 0), (CHUNKS + 3, 1)):
            @pl.when(i == at)
            def _():
                arrive_first(job)
                arrive_inner(job)

        upper, lower = split(dot(x_buf[c], basis[k]))
        for n in range(4):
            cot = cot_buf[k, c, :, n * width : (n + 1) * width]
            acc[k, n] += dot_first(upper, cot) + dot_first(lower, cot)
        return carry

    lax.fori_loop(0, 2 * CHUNKS, one_step, 0)
    s1(1).start()

    plan = []

    def at(time, job, *args):
        plan.append((time, len(plan), job, args))

    beat = 2.85
    for i in range(count):
        if i > 1:
            at(5 + beat * (i + 1), arrive_first, i)
            at(5.1 + beat * (i + 1), arrive_inner, i)
        at(8 + beat * (count + i + 1), arrive_second, i)
        at(14 + beat * (2 * count + i + 1), arrive_third, i)
    for c in range(4):
        at(14 + beat * (c + 1), relay, 1, c)
        at(17 + beat * (count + c + 1), relay, 2, c)
        at(23 + beat * (2 * count + c + 1), relay, 3, c)
    at(13, make_gram)
    for k in range(2):
        lag = 5 * k
        at(17 + lag, halve, k)
        at(23 + lag, quarter, k)
        at(31 + lag, update, k)
        at(38 + lag, collect, k)
        at(44 + lag, collect_second, k)
        at(52 + lag, measure, k)
    for _, _, job, args in sorted(plan, key=lambda entry: entry[:2]):
        job(*args)

    q4 = send(sq_buf.at[0], sq_buf.at[1], q_send, q_recv, tp=1 - t)
    q4.start()
    for k in range(2):
        for stage in (1, 2):
            p4(k, stage).wait_recv()
    for slot in (1, 2, 3):
        for c in range(4):
            if c not in RELAY_X:
                to_y(slot, c).wait_recv()
            else:
                relay_x(slot, c).wait_recv()
                relay_x(slot, c).wait_send()
            if c not in RELAY_Y:
                to_x(slot, c).wait_recv()
            else:
                relay_y(slot, c).wait_recv()
                relay_y(slot, c).wait_send()
            to_x(slot, c).wait_send()
            to_y(slot, c).wait_send()
    for i in range(count):
        own_ahead(i).wait_send()

        @pl.when(inner)
        def _():
            own_behind(i).wait_send()
            for slot in (1, 2, 3):
                pass_along(slot, i).wait_send()
    for k in range(2):
        s1(k).wait_send()
        s2(k).wait_send()
        for d in range(1, n_fs):
            s3(k, d).wait_send()
            a4(k, d).wait_send()
        for stage in range(3):
            g4(k, stage).wait_send()
            p4(k, stage).wait_send()
    for o in range(2 if EXTRA else 1, 4):
        for k in range(2):
            w_load(o, k).wait()
    q4.wait()
    squares_out[...] = sq_buf[0] + sq_buf[1]


def finish_block(
    entries, gathered, scaled, proj, squares, basis, weight, moments,
    value_new, gate_new, value_copy, gate_copy, value_step, gate_step,
    value_first_new, gate_first_new, value_second_new, gate_second_new,
    new_buf, step_buf, copy_buf, moment_buf, new_sem, step_sem, copy_sem, moment_sem,
):
    f = lax.axis_index("fs")
    rows = weight.shape[1]
    model = gathered.shape[1]
    width = scaled.shape[3]
    block = min(rows, 256)
    own = rows // block
    blocks = model // block
    news, copies, steps = (value_new, gate_new), (value_copy, gate_copy), (value_step, gate_step)
    factors = [lax.rsqrt(squares[k, :1, :1] / entries + 1e-06) for k in range(2)]

    def span(start, size):
        return pl.ds(pl.multiple_of(start, size), size)

    def row_of(b):
        return lax.rem(f * own + b, blocks) * block

    def new_out(k, b):
        return pltpu.make_async_copy(
            new_buf.at[k, span(b * block, block)], news[k].at[span(b * block, block)], new_sem.at[k, b])

    def step_store(k, b):
        return pltpu.make_async_copy(
            step_buf.at[k, span(b * block, block)], steps[k].at[span(b * block, block)], step_sem.at[k, b])

    def copy_out(k, b):
        where = span(row_of(b), block)
        return pltpu.make_async_copy(copy_buf.at[k, where], copies[k].at[where], copy_sem.at[k, b])

    def own_block(b, carry):
        for k in range(2):
            where = span(row_of(b), block)
            local_rows = span(b * block, block)
            for n in range(4):
                cols = slice(n * width, (n + 1) * width)
                direction = dot(basis[k, where], scaled[k, n]) * factors[k]
                updated = weight[k, local_rows, cols] - learn_rate * direction
                step_buf[k, local_rows, cols] = direction
                new_buf[k, local_rows, cols] = updated
                copy_buf[k, where, cols] = updated.astype(BF16)
            step_store(k, b).start()
            new_out(k, b).start()
            copy_out(k, b).start()
        return carry

    lax.fori_loop(0, own, own_block, 0)
    outs = (value_first_new, gate_first_new, value_second_new, gate_second_new)
    for k in range(2):
        for n in range(4):
            cols = slice(n * width, (n + 1) * width)
            small = proj[k, n]
            moment_buf[k, :, cols] = 0.9 * moments[k, :, cols] + 0.1 * small
            moment_buf[2 + k, :, cols] = 0.95 * moments[2 + k, :, cols] + 0.05 * small * small
    moment_outs = [pltpu.make_async_copy(moment_buf.at[i], outs[i], moment_sem.at[i]) for i in range(4)]
    for copy in moment_outs:
        copy.start()

    def other_block(b, carry):
        for k in range(2):
            where = span(row_of(b), block)
            for n in range(4):
                cols = slice(n * width, (n + 1) * width)
                direction = dot(basis[k, where], scaled[k, n]) * (learn_rate * factors[k])
                copy_buf[k, where, cols] = (gathered[k, where, cols].astype(F32) - direction).astype(BF16)
            copy_out(k, b).start()
        return carry

    lax.fori_loop(own, blocks, other_block, 0)

    def drain_own(b, carry):
        for k in range(2):
            step_store(k, b).wait()
            new_out(k, b).wait()
        return carry

    def drain(b, carry):
        for k in range(2):
            copy_out(k, b).wait()
        return carry

    lax.fori_loop(0, own, drain_own, 0)
    lax.fori_loop(0, blocks, drain, 0)
    for copy in moment_outs:
        copy.wait()


def local_block(*args):
    (mixer, value_cot, gate_cot, value_weight, gate_weight, value_basis, gate_basis,
     value_first, gate_first, value_second, gate_second) = args
    n_fs = 4
    tokens, model = mixer.shape
    half = value_cot.shape[1]
    rows = value_weight.shape[0]
    rank = value_basis.shape[1]
    low = value_first.shape[0]
    width = half // 4
    chunk = tokens // CHUNKS
    count = 4 + len(EXTRA)
    hbm = pl.BlockSpec(memory_space=pltpu.HBM)
    vmem = pl.BlockSpec(memory_space=pltpu.VMEM)
    dma = pltpu.SemaphoreType.DMA
    scratch = [
        pltpu.VMEM((CHUNKS, chunk, model), BF16),
        pltpu.VMEM((2, CHUNKS, chunk, half), BF16),
        pltpu.VMEM((2, 2, rank, rank), BF16),
        pltpu.VMEM((2, 4, rank, width), F32),
        pltpu.VMEM((2, 2, rank, width), F32),
        pltpu.VMEM((2, rank, width), F32),
        pltpu.VMEM((2, rank, width), F32),
        pltpu.VMEM((2, rank, width), F32),
        pltpu.VMEM((2, n_fs - 1, low, width), F32),
        pltpu.VMEM((2, 2, 8, 128), F32),
        dma((CHUNKS,)), dma((2, CHUNKS)), dma((2,)), dma((4, 2)), dma((4,)),
        dma((5, count)), dma((3, count)),
    ]
    scratch += [dma((3, 4)) for _ in range(8)]
    scratch += [dma((2,)) for _ in range(4)]
    scratch += [dma((2, 3)) for _ in range(8)]
    scratch += [dma(()), dma(())]
    outs = pl.pallas_call(
        exchange_block,
        out_shape=(
            pltpu.VMEM((2, model, half), BF16),
            pltpu.VMEM((2, 4, rank, width), BF16),
            pltpu.VMEM((2, 4, low, width), F32),
            pltpu.VMEM((2, 8, 128), F32),
            pltpu.VMEM((2, model, rank), BF16),
            pltpu.VMEM((2, rows, half), F32),
            pltpu.VMEM((4, low, half), F32),
        ),
        in_specs=[hbm] * 11,
        out_specs=(vmem,) * 7,
        scratch_shapes=scratch,
        compiler_params=pltpu.CompilerParams(
            collective_id=0, has_side_effects=True, vmem_limit_bytes=VMEM_FIRST
        ),
        name="exchange_block",
    )(*args)
    outs = [pltpu.with_memory_space_constraint(out, pltpu.VMEM) for out in outs]
    block = min(rows, 256)
    return pl.pallas_call(
        functools.partial(finish_block, float(model) * half * 2),
        in_specs=[vmem] * 7,
        out_specs=[hbm] * 10,
        out_shape=[
            jax.ShapeDtypeStruct((rows, half), F32),
            jax.ShapeDtypeStruct((rows, half), F32),
            jax.ShapeDtypeStruct((model, half), BF16),
            jax.ShapeDtypeStruct((model, half), BF16),
            jax.ShapeDtypeStruct((rows, half), F32),
            jax.ShapeDtypeStruct((rows, half), F32),
        ] + [jax.ShapeDtypeStruct((low, half), F32)] * 4,
        scratch_shapes=[
            pltpu.VMEM((2, rows, half), F32),
            pltpu.VMEM((2, rows, half), F32),
            pltpu.VMEM((2, model, half), BF16),
            pltpu.VMEM((4, low, half), F32),
            dma((2, rows // block)), dma((2, rows // block)), dma((2, model // block)), dma((4,)),
        ],
        compiler_params=pltpu.CompilerParams(vmem_limit_bytes=VMEM_SECOND),
        name="finish_block",
    )(*outs)


def solution(mesh):
    sizes = tuple(mesh.shape[name] for name in ("fs", "rep", "tp"))
    return jax.shard_map(
        lambda *args: tuple(local_block(*args) if sizes == (4, 4, 2) else local(sizes, *args)),
        mesh=mesh,
        in_specs=(
            P(("fs", "rep"), None),
            P(("fs", "rep"), "tp"),
            P(("fs", "rep"), "tp"),
            P("fs", "tp"),
            P("fs", "tp"),
            P(),
            P(),
            P("fs", "tp"),
            P("fs", "tp"),
            P("fs", "tp"),
            P("fs", "tp"),
        ),
        out_specs=(
            P("fs", "tp"),
            P("fs", "tp"),
            P(None, "tp"),
            P(None, "tp"),
            P("fs", "tp"),
            P("fs", "tp"),
            P("fs", "tp"),
            P("fs", "tp"),
            P("fs", "tp"),
            P("fs", "tp"),
        ),
        check_vma=False,
    )
```

```python
import functools

import jax
import jax.numpy as jnp
from jax import lax
from jax.experimental import pallas as pl
from jax.experimental.pallas import tpu as pltpu
from jax.sharding import PartitionSpec as P

learn_rate = 0.02
CHUNKS = 4
VMEM_FIRST = 40 * 1024 * 1024
VMEM_SECOND = 40 * 1024 * 1024
F32 = jnp.float32
BF16 = jnp.bfloat16


def dot(a, b):
    return jnp.dot(a, b, preferred_element_type=F32)


def dot_first(a, b):
    return lax.dot_general(a, b, (((0,), (0,)), ((), ())), preferred_element_type=F32)


def split(a):
    upper = a.astype(BF16)
    return upper, (a - upper.astype(F32)).astype(BF16)


def exchange(
    n_fs, n_rep, n_tp,
    mixer, value_cot, gate_cot, value_weight, gate_weight, value_basis, gate_basis,
    value_first_hbm, gate_first_hbm, value_second_hbm, gate_second_hbm,
    value_rows, gate_rows, scaled_out, projected_out, squares_out,
    x_buf, cot_buf, w_buf, w_half, basis_buf, gram, acc, part_in,
    mid, mid_in, proj_all, scaled, sq_buf, moments,
    x_sem, w_sem, b_sem, own_sem, m_sem,
    w1_send, w1_recv, w2_send, w2_recv,
    s1_send, s1_recv, s2_send, s2_recv, p_send, p_recv, a_send, a_recv, g_send, g_recv, q_send, q_recv,
):
    f, r, t = lax.axis_index("fs"), lax.axis_index("rep"), lax.axis_index("tp")
    cots = (value_cot, gate_cot)
    weights = (value_weight, gate_weight)
    bases = (value_basis, gate_basis)
    gathered = (value_rows, gate_rows)
    tokens = mixer.shape[0]
    chunk = tokens // CHUNKS
    rows = value_weight.shape[0]
    share = rows // n_rep
    width = acc.shape[2]
    per_role = n_rep // 2
    low = mid.shape[1]

    def fs_at(d):
        return lax.rem(f + d, n_fs)

    def rep_at(d):
        return lax.rem(r + d, n_rep)

    def send(src, dst, s, v, **where):
        return pltpu.make_async_remote_copy(
            src_ref=src, dst_ref=dst, send_sem=s, recv_sem=v,
            device_id=where, device_id_type=pl.DeviceIdType.MESH,
        )

    w_loads = [pltpu.make_async_copy(weights[k], w_buf.at[k], w_sem.at[k]) for k in range(2)]
    b_loads = [pltpu.make_async_copy(bases[k], basis_buf.at[k], b_sem.at[k]) for k in range(2)]

    def x_loads(c):
        span = pl.ds(pl.multiple_of(c * chunk, chunk), chunk)
        return [pltpu.make_async_copy(mixer.at[span], x_buf.at[c], x_sem.at[c, 0])] + [
            pltpu.make_async_copy(cots[k].at[span], cot_buf.at[k, c], x_sem.at[c, 1 + k]) for k in range(2)
        ]

    m_loads = [
        pltpu.make_async_copy(ref, moments.at[i], m_sem.at[i])
        for i, ref in enumerate((value_first_hbm, gate_first_hbm, value_second_hbm, gate_second_hbm))
    ]
    for copy in w_loads + b_loads:
        copy.start()
    for c in range(CHUNKS):
        for copy in x_loads(c):
            copy.start()

    for copy in m_loads:
        copy.start()

    barrier = pltpu.get_barrier_semaphore()
    for d in range(1, n_fs):
        pl.semaphore_signal(barrier, inc=1, device_id={"fs": fs_at(d)}, device_id_type=pl.DeviceIdType.MESH)
    for d in range(1, n_rep):
        pl.semaphore_signal(barrier, inc=1, device_id={"rep": rep_at(d)}, device_id_type=pl.DeviceIdType.MESH)
    for d in range(1, n_tp):
        pl.semaphore_signal(
            barrier, inc=1, device_id={"tp": lax.rem(t + d, n_tp)}, device_id_type=pl.DeviceIdType.MESH
        )
    for k in range(2):
        w_loads[k].wait()
        w_half[k] = w_buf[k].astype(BF16)
    pl.semaphore_wait(barrier, n_fs + n_rep + n_tp - 3)

    def share_of(block, part_index):
        return pl.ds(pl.multiple_of(block * rows + part_index * share, share), share)

    w1 = {}
    for d in range(1, n_fs):
        for k in range(2):
            w1[d, k] = send(
                w_half.at[k, pl.ds(pl.multiple_of(r * share, share), share)],
                gathered[k].at[share_of(f, r)],
                w1_send.at[d - 1, k], w1_recv.at[d - 1, k], fs=fs_at(d),
            )
            w1[d, k].start()
    own = []
    for k in range(2):
        copy = pltpu.make_async_copy(
            w_half.at[k], gathered[k].at[pl.ds(pl.multiple_of(f * rows, rows), rows)], own_sem.at[k]
        )
        copy.start()
        own.append(copy)

    for copy in b_loads:
        copy.wait()
    acc[...] = jnp.zeros_like(acc)

    def one_chunk(c, carry):
        for copy in x_loads(c):
            copy.wait()
        x = x_buf[c]
        for k in range(2):
            upper, lower = split(dot(x, basis_buf[k]))
            for q in range(per_role):
                cols = slice(q * width, (q + 1) * width)
                cot = cot_buf[k, c, :, cols]
                acc[k * per_role + q] += dot_first(upper, cot) + dot_first(lower, cot)
        return carry

    lax.fori_loop(0, CHUNKS, one_chunk, 0)
    s1 = {}
    for d in range(1, n_rep):
        s1[d] = send(
            acc.at[rep_at(d)], part_in.at[d - 1], s1_send.at[d - 1], s1_recv.at[d - 1], rep=rep_at(d)
        )
        s1[d].start()

    w2, heard = {}, set()
    near, far = (r + 1 - 2 * lax.rem(r, 2), lax.rem(r + 2, n_rep)) if n_rep == 4 else (None, None)

    def pass_on(d, e, k, owner, peer):
        source = lax.rem(f - d + n_fs, n_fs)
        rows_ref = gathered[k].at[share_of(source, owner)]
        w2[d, e, k] = send(
            rows_ref, rows_ref, w2_send.at[d - 1, e, k], w2_recv.at[d - 1, e, k], rep=peer
        )
        w2[d, e, k].start()

    def forward(d):
        for k in range(2):
            w1[d, k].wait_recv()
            peers = (near, far) if n_rep == 4 else [rep_at(e) for e in range(1, n_rep)]
            for e, peer in enumerate(peers):
                pass_on(d, e, k, r, peer)

    def relay(d):
        if n_rep == 4:
            for e, k, owner, peer in ((0, 0, near, far), (1, 1, far, near)):
                w2[d, e, k].wait_recv()
                heard.add((d, e, k))
                pass_on(d, 2, k, owner, peer)

    forward(1)
    for k in range(2):
        upper, lower = split(dot_first(basis_buf[k], basis_buf[k]))
        gram[k, 0] = upper
        gram[k, 1] = lower

    for d in range(1, n_rep):
        s1[d].wait_recv()
    total = acc[r]
    for d in range(1, n_rep):
        total += part_in[d - 1]
    mid[...] = total.reshape(mid.shape)
    s2 = {}
    for d in range(1, n_fs):
        s2[d] = send(
            mid.at[fs_at(d)], mid_in.at[d - 1], s2_send.at[d - 1], s2_recv.at[d - 1], fs=fs_at(d)
        )
        s2[d].start()
    for d in range(2, n_fs - 1):
        forward(d)
        relay(d - 1)
    for d in range(1, n_fs):
        s2[d].wait_recv()
    small = mid[f]
    for d in range(1, n_fs):
        small += mid_in[d - 1]
    proj_all[r] = small.astype(BF16)

    cols = pl.ds(pl.multiple_of(lax.rem(r, per_role) * width, width), width)
    is_value = r < per_role
    for copy in m_loads:
        copy.wait()
    first = jnp.where(is_value, moments[0, :, cols], moments[1, :, cols])
    second = jnp.where(is_value, moments[2, :, cols], moments[3, :, cols])
    first_new = 0.9 * first + 0.1 * small
    second_new = 0.95 * second + 0.05 * small * small
    scaled[r, f] = (first_new * lax.rsqrt(second_new)).astype(BF16)
    a4, p4, g4 = {}, {}, {}
    for d in range(1, n_fs):
        a4[d] = send(
            scaled.at[r, f], scaled.at[r, f], a_send.at[d - 1], a_recv.at[d - 1], fs=fs_at(d)
        )
        a4[d].start()
    for d in range(1, n_rep):
        p4[d] = send(proj_all.at[r], proj_all.at[r], p_send.at[d - 1], p_recv.at[d - 1], rep=rep_at(d))
        p4[d].start()
    if n_fs > 2:
        forward(n_fs - 1)
        relay(n_fs - 2)
    for d in range(1, n_fs):
        a4[d].wait_recv()
    for d in range(1, n_rep):
        g4[d] = send(scaled.at[r], scaled.at[r], g_send.at[d - 1], g_recv.at[d - 1], rep=rep_at(d))
        g4[d].start()
    relay(n_fs - 1)
    for d in range(1, n_rep):
        g4[d].wait_recv()

    for k in range(2):
        squares = 0.0
        for q in range(per_role):
            s = scaled[k * per_role + q].reshape(n_fs * low, width)
            squares += jnp.sum((dot(gram[k, 0], s) + dot(gram[k, 1], s)) * s.astype(F32))
        sq_buf[0, k] = jnp.full(sq_buf.shape[2:], squares, F32)
    q4 = []
    for d in range(1, n_tp):
        copy = send(
            sq_buf.at[0], sq_buf.at[d], q_send.at[d - 1], q_recv.at[d - 1], tp=lax.rem(t + d, n_tp)
        )
        copy.start()
        q4.append(copy)
    for d in range(1, n_rep):
        p4[d].wait_recv()
    scaled_out[...] = scaled[...].reshape(scaled_out.shape)
    projected_out[...] = proj_all[...]
    for copy in q4:
        copy.wait_recv()
    sums = sq_buf[0]
    for d in range(1, n_tp):
        sums += sq_buf[d]
    squares_out[...] = sums

    for copy in list(w1.values()) + list(s1.values()) + list(s2.values()) + list(a4.values()):
        copy.wait_send()
    for copy in list(p4.values()) + list(g4.values()) + q4:
        copy.wait_send()
    for copy in own:
        copy.wait()
    for key, copy in w2.items():
        copy.wait_send()
        if key not in heard:
            copy.wait_recv()


def finish(
    own_blocks, entries,
    where, value_rows, gate_rows, value_basis, gate_basis, value_weight, gate_weight,
    scaled, projected, squares, value_first, gate_first, value_second, gate_second,
    value_new, gate_new, value_copy, gate_copy, value_step, gate_step,
    value_first_new, gate_first_new, value_second_new, gate_second_new,
):
    step = pl.program_id(0)
    width = scaled.shape[2]
    per_role = scaled.shape[0] // 2
    roles = (
        (value_rows, value_basis, value_weight, value_new, value_copy, value_step),
        (gate_rows, gate_basis, gate_weight, gate_new, gate_copy, gate_step),
    )
    for k, (rows, basis, weight, new, copy, step_out) in enumerate(roles):
        factor = lax.rsqrt(squares[k, :1, :1] / entries + 1e-06)
        for q in range(per_role):
            cols = slice(q * width, (q + 1) * width)
            direction = dot(basis[...], scaled[k * per_role + q]) * factor
            copy[:, cols] = (rows[:, cols].astype(F32) - learn_rate * direction).astype(BF16)

            @pl.when(step < own_blocks)
            def _():
                step_out[:, cols] = direction
                new[:, cols] = weight[:, cols] - learn_rate * direction

    @pl.when(step == 0)
    def _():
        moments = (
            (value_first, value_second, value_first_new, value_second_new),
            (gate_first, gate_second, gate_first_new, gate_second_new),
        )
        for k, (first, second, first_new, second_new) in enumerate(moments):
            for q in range(per_role):
                cols = slice(q * width, (q + 1) * width)
                small = projected[k * per_role + q].astype(F32)
                first_new[:, cols] = 0.9 * first[:, cols] + 0.1 * small
                second_new[:, cols] = 0.95 * second[:, cols] + 0.05 * small * small


def local(sizes, *args):
    n_fs, n_rep, n_tp = sizes
    (mixer, value_cot, gate_cot, value_weight, gate_weight, value_basis, gate_basis,
     value_first, gate_first, value_second, gate_second) = args
    tokens, model = mixer.shape
    half = value_cot.shape[1]
    rows = value_weight.shape[0]
    rank = value_basis.shape[1]
    low = value_first.shape[0]
    width = 2 * half // n_rep
    chunk = tokens // CHUNKS
    any_spec = pl.BlockSpec(memory_space=pl.ANY)
    vmem = pl.BlockSpec(memory_space=pltpu.VMEM)
    dma = pltpu.SemaphoreType.DMA
    scratch = [
        pltpu.VMEM((CHUNKS, chunk, model), BF16),
        pltpu.VMEM((2, CHUNKS, chunk, half), BF16),
        pltpu.VMEM((2, rows, half), F32),
        pltpu.VMEM((2, rows, half), BF16),
        pltpu.VMEM((2, model, rank), BF16),
        pltpu.VMEM((2, 2, rank, rank), BF16),
        pltpu.VMEM((n_rep, rank, width), F32),
        pltpu.VMEM((n_rep - 1, rank, width), F32),
        pltpu.VMEM((n_fs, low, width), F32),
        pltpu.VMEM((n_fs - 1, low, width), F32),
        pltpu.VMEM((n_rep, low, width), BF16),
        pltpu.VMEM((n_rep, n_fs, low, width), BF16),
        pltpu.VMEM((n_tp, 2, 8, 128), F32),
        pltpu.VMEM((4, low, half), F32),
        dma((CHUNKS, 3)), dma((2,)), dma((2,)), dma((2,)), dma((4,)),
        dma((n_fs - 1, 2)), dma((n_fs - 1, 2)),
        dma((n_fs - 1, n_rep - 1, 2)), dma((n_fs - 1, n_rep - 1, 2)),
    ]
    for count in (n_rep, n_fs, n_rep, n_fs, n_rep, n_tp):
        scratch += [dma((count - 1,)), dma((count - 1,))]
    value_rows, gate_rows, scaled, projected, squares = pl.pallas_call(
        functools.partial(exchange, n_fs, n_rep, n_tp),
        out_shape=(
            jax.ShapeDtypeStruct((rows * n_fs, half), BF16),
            jax.ShapeDtypeStruct((rows * n_fs, half), BF16),
            jax.ShapeDtypeStruct((n_rep, rank, width), BF16),
            jax.ShapeDtypeStruct((n_rep, low, width), BF16),
            jax.ShapeDtypeStruct((2, 8, 128), F32),
        ),
        in_specs=[any_spec] * 11,
        out_specs=(any_spec, any_spec, vmem, vmem, vmem),
        scratch_shapes=scratch,
        compiler_params=pltpu.CompilerParams(
            collective_id=0, has_side_effects=True, vmem_limit_bytes=52 * 1024 * 1024
        ),
        name="exchange",
    )(*args)

    block = min(rows, 256)
    own_blocks = rows // block
    blocks = model // block
    where = (lax.axis_index("fs") * own_blocks).astype(jnp.int32).reshape(1)

    def turned(i, w):
        return (lax.rem(w[0] + i, blocks), 0)

    def own(i, w):
        return (jnp.minimum(i, own_blocks - 1), 0)

    def whole(shape):
        return pl.BlockSpec(shape, lambda i, w: (0,) * len(shape))

    row_spec = pl.BlockSpec((block, half), turned)
    basis_spec = pl.BlockSpec((block, rank), turned)
    own_spec = pl.BlockSpec((block, half), own)
    moment = whole((low, half))
    return pl.pallas_call(
        functools.partial(finish, own_blocks, float(model) * half * n_tp),
        grid_spec=pltpu.PrefetchScalarGridSpec(
            num_scalar_prefetch=1,
            grid=(blocks,),
            in_specs=[row_spec, row_spec, basis_spec, basis_spec, own_spec, own_spec,
                      whole(scaled.shape), whole(projected.shape), whole(squares.shape)] + [moment] * 4,
            out_specs=[own_spec, own_spec, row_spec, row_spec, own_spec, own_spec] + [moment] * 4,
        ),
        out_shape=[
            jax.ShapeDtypeStruct((rows, half), F32),
            jax.ShapeDtypeStruct((rows, half), F32),
            jax.ShapeDtypeStruct((model, half), BF16),
            jax.ShapeDtypeStruct((model, half), BF16),
            jax.ShapeDtypeStruct((rows, half), F32),
            jax.ShapeDtypeStruct((rows, half), F32),
        ] + [jax.ShapeDtypeStruct((low, half), F32)] * 4,
        compiler_params=pltpu.CompilerParams(vmem_limit_bytes=40 * 1024 * 1024),
        name="finish",
    )(where, value_rows, gate_rows, value_basis, gate_basis, value_weight, gate_weight,
      scaled, projected, squares, value_first, gate_first, value_second, gate_second)


EXTRA = (0, 1)
RELAY_X = (2,)
RELAY_Y = (3,)
EARLY = (
    (2, "relay", 2, 0), (2, "first", 0), (4, "begin", 0), (4, "relay", 1, 0), (4, "first", 1),
    (6, "first", 2),
)
LATE = (
    ("relay", 3, 1), ("inner", 0), ("begin", 1), ("inner", 2), ("inner", 3), ("halve", 0), ("first", 3),
    ("second", 2), ("halve", 1), ("inner", 1), ("third", 2), ("second", 3), ("gram",), ("relay", 1, 2),
    ("relay", 1, 3), ("quarter", 0), ("relay", 3, 0), ("second", 0), ("second", 1), ("relay", 1, 1),
    ("quarter", 1), ("third", 0), ("update", 0), ("inner", 4), ("inner", 5), ("update", 1), ("third", 1),
    ("collect", 0), ("first", 4), ("third", 3), ("collect", 1), ("second", 4), ("again", 0), ("relay", 3, 3),
    ("relay", 3, 2), ("relay", 2, 2), ("again", 1), ("first", 5), ("relay", 2, 3), ("relay", 2, 1),
    ("second", 5), ("measure", 0), ("third", 4), ("measure", 1), ("third", 5),
)


def exchange_block(
    mixer, value_cot, gate_cot, value_weight, gate_weight, value_basis, gate_basis,
    value_first, gate_first, value_second, gate_second,
    gathered, scaled, proj, squares_out, basis, weight, moments,
    x_buf, cot_buf, gram, acc, first_in, second_out, second_in, part, part_in, sq_buf,
    x_sem, c_sem, b_sem, w_sem, m_sem,
    z_send, z_recv, x_send, x_recv, y_send, y_recv, rx_send, rx_recv, ry_send, ry_recv,
    s1_send, s1_recv, s2_send, s2_recv, s3_send, s3_recv, a_send, a_recv,
    g_send, g_recv, p_send, p_recv, q_send, q_recv,
):
    f, r, t = lax.axis_index("fs"), lax.axis_index("rep"), lax.axis_index("tp")
    n_fs = 4
    cots = (value_cot, gate_cot)
    weights = (value_weight, gate_weight)
    bases = (value_basis, gate_basis)
    tokens = mixer.shape[0]
    chunk = tokens // CHUNKS
    rows = value_weight.shape[0]
    share = rows // 4
    piece_rows = share // 2
    low = moments.shape[1]
    width = acc.shape[3]
    ends = jnp.logical_or(f == 0, f == n_fs - 1)
    inner = jnp.logical_not(ends)
    turn = 1 - 2 * (f // 2)
    ahead = f + turn
    behind = jnp.clip(f - turn, 0, n_fs - 1)
    x_at, y_at = lax.rem(r, 2), r // 2
    x_peer, y_peer = r + 1 - 2 * x_at, r + 2 - 4 * y_at
    across = 3 - r
    half_at, part_at = (x_at, y_at), (y_at, x_at)
    half_peer, part_peer = (x_peer, y_peer), (y_peer, x_peer)
    mine = [2 * half_at[k] + part_at[k] for k in range(2)]

    def fs_at(d):
        return lax.rem(f + d, n_fs)

    def send(src, dst, s, v, **where):
        return pltpu.make_async_remote_copy(
            src_ref=src, dst_ref=dst, send_sem=s, recv_sem=v,
            device_id=where, device_id_type=pl.DeviceIdType.MESH,
        )

    def span(start, size):
        return pl.ds(pl.multiple_of(start, size), size)

    def piece(plane, quarter, c):
        return gathered.at[c % 2, span(plane * rows + quarter * share + (c // 2) * piece_rows, piece_rows)]

    z_pieces = [(r, c) for c in range(4)] + [(across, c) for c in EXTRA]
    count = len(z_pieces)
    order = (r, across, x_peer, y_peer)

    def w_load(o, k):
        where = span(order[o] * share, share)
        return pltpu.make_async_copy(weights[k].at[where], weight.at[k, where], w_sem.at[o, k])

    def b_load(k):
        return pltpu.make_async_copy(bases[k], basis.at[k], b_sem.at[k])

    def x_load(c):
        return pltpu.make_async_copy(mixer.at[span(c * chunk, chunk)], x_buf.at[c], x_sem.at[c])

    def c_load(k, c):
        return pltpu.make_async_copy(cots[k].at[span(c * chunk, chunk)], cot_buf.at[k, c], c_sem.at[k, c])

    m_loads = [
        pltpu.make_async_copy(ref, moments.at[i], m_sem.at[i])
        for i, ref in enumerate((value_first, gate_first, value_second, gate_second))
    ]
    for k in range(2):
        w_load(0, k).start()
    if EXTRA:
        for k in range(2):
            w_load(1, k).start()
    b_load(0).start()
    for c in range(CHUNKS):
        x_load(c).start()
        c_load(0, c).start()
    b_load(1).start()
    for c in range(CHUNKS):
        c_load(1, c).start()
    for copy in m_loads:
        copy.start()
    for o in range(2 if EXTRA else 1, 4):
        for k in range(2):
            w_load(o, k).start()

    barrier = pltpu.get_barrier_semaphore()
    for d in range(1, n_fs):
        pl.semaphore_signal(barrier, inc=1, device_id={"fs": fs_at(d)}, device_id_type=pl.DeviceIdType.MESH)
    for peer in (x_peer, y_peer):
        pl.semaphore_signal(barrier, inc=1, device_id={"rep": peer}, device_id_type=pl.DeviceIdType.MESH)
    pl.semaphore_signal(barrier, inc=1, device_id={"tp": 1 - t}, device_id_type=pl.DeviceIdType.MESH)

    for o in range(2 if EXTRA else 1):
        where = span(order[o] * share, share)
        for k in range(2):
            w_load(o, k).wait()
            gathered[k, span(f * rows + order[o] * share, share)] = weight[k, where].astype(BF16)
    pl.semaphore_wait(barrier, n_fs + 2)

    def plane_of(slot):
        return lax.rem(f + turn * slot + n_fs, n_fs)

    landing = jnp.where(ends, 2, 0)

    def own_ahead(i):
        quarter, c = z_pieces[i]
        ref = piece(f, quarter, c)
        return send(ref, ref, z_send.at[0, i], z_recv.at[landing, i], fs=ahead)

    def own_behind(i):
        quarter, c = z_pieces[i]
        ref = piece(f, quarter, c)
        return send(ref, ref, z_send.at[1, i], z_recv.at[0, i], fs=behind)

    def pass_along(slot, i):
        quarter, c = z_pieces[i]
        ref = piece(plane_of(slot), quarter, c)
        if slot == 3:
            return send(ref, ref, z_send.at[4, i], z_recv.at[1, i], fs=ahead)
        return send(ref, ref, z_send.at[1 + slot, i], z_recv.at[slot, i], fs=behind)

    def arrival(slot, i):
        quarter, c = z_pieces[i]
        ref = piece(plane_of(slot), quarter, c)
        return send(ref, ref, z_send.at[0, i], z_recv.at[slot - 1, i], fs=ahead)

    for i in range(count):
        own_ahead(i).start()

        @pl.when(inner)
        def _():
            own_behind(i).start()

    def to_x(slot, c):
        ref = piece(plane_of(slot), r, c)
        return send(ref, ref, x_send.at[slot - 1, c], x_recv.at[slot - 1, c], rep=x_peer)

    def to_y(slot, c):
        ref = piece(plane_of(slot), r, c)
        return send(ref, ref, y_send.at[slot - 1, c], y_recv.at[slot - 1, c], rep=y_peer)

    def relay_x(slot, c):
        ref = piece(plane_of(slot), y_peer, c)
        return send(ref, ref, rx_send.at[slot - 1, c], rx_recv.at[slot - 1, c], rep=x_peer)

    def relay_y(slot, c):
        ref = piece(plane_of(slot), x_peer, c)
        return send(ref, ref, ry_send.at[slot - 1, c], ry_recv.at[slot - 1, c], rep=y_peer)

    def spread(slot, i):
        if i < 4:
            to_x(slot, i).start()
            to_y(slot, i).start()

    def arrive_first(i):
        arrival(1, i).wait_recv()

        @pl.when(inner)
        def _():
            pass_along(1, i).start()

        spread(1, i)

    def arrive_inner(i):
        @pl.when(inner)
        def _():
            arrival(3, i).wait_recv()
            pass_along(3, i).start()

    def arrive_second(i):
        arrival(2, i).wait_recv()

        @pl.when(inner)
        def _():
            pass_along(2, i).start()

        spread(2, i)

    def arrive_third(i):
        @pl.when(ends)
        def _():
            arrival(3, i).wait_recv()

        spread(3, i)

    def relay(slot, c):
        if c in RELAY_X:
            to_y(slot, c).wait_recv()
            relay_x(slot, c).start()
        if c in RELAY_Y:
            to_x(slot, c).wait_recv()
            relay_y(slot, c).start()

    def s1(k):
        other = acc.at[k, pl.ds(2 * (1 - half_at[k]), 2)]
        return send(other, first_in.at[k], s1_send.at[k], s1_recv.at[k], rep=half_peer[k])

    def s2(k):
        return send(second_out.at[k], second_in.at[k], s2_send.at[k], s2_recv.at[k], rep=part_peer[k])

    def s3(k, d):
        return send(
            part.at[k, span(fs_at(d) * low, low)], part_in.at[k, d - 1],
            s3_send.at[k, d - 1], s3_recv.at[k, d - 1], fs=fs_at(d),
        )

    def halve(k):
        s1(k).wait_recv()
        other = 1 - part_at[k]
        second_out[k] = acc[k, 2 * half_at[k] + other] + first_in[k, other]
        s2(k).start()
        part[k] = acc[k, mine[k]] + first_in[k, part_at[k]]

    def quarter(k):
        s2(k).wait_recv()
        part[k] += second_in[k]
        for d in range(1, n_fs):
            s3(k, d).start()

    def a4(k, d):
        ref = scaled.at[k, mine[k], span(f * low, low)]
        return send(ref, ref, a_send.at[k, d - 1], a_recv.at[k, d - 1], fs=fs_at(d))

    def grow(buf, ss, vs, k, stage):
        if stage == 0:
            ref = buf.at[k, mine[k]]
            return send(ref, ref, ss.at[k, 0], vs.at[k, 0], rep=part_peer[k])
        if stage == 1:
            ref = buf.at[k, mine[k]]
            return send(ref, ref, ss.at[k, 1], vs.at[k, 1], rep=half_peer[k])
        ref = buf.at[k, 2 * half_at[k] + 1 - part_at[k]]
        return send(ref, ref, ss.at[k, 2], vs.at[k, 2], rep=half_peer[k])

    def g4(k, stage):
        return grow(scaled, g_send, g_recv, k, stage)

    def p4(k, stage):
        return grow(proj, p_send, p_recv, k, stage)

    def update(k):
        if k == 0:
            for copy in m_loads:
                copy.wait()
        for d in range(1, n_fs):
            s3(k, d).wait_recv()
        small = part[k, span(f * low, low)]
        for d in range(1, n_fs):
            small += part_in[k, d - 1]
        proj[k, mine[k]] = small.astype(BF16)
        cols = span(mine[k] * width, width)
        first_new = 0.9 * moments[k, :, cols] + 0.1 * small
        second_new = 0.95 * moments[2 + k, :, cols] + 0.05 * small * small
        scaled[k, mine[k], span(f * low, low)] = (first_new * lax.rsqrt(second_new)).astype(BF16)
        for d in range(1, n_fs):
            a4(k, d).start()

    def collect(k):
        for d in range(1, n_fs):
            a4(k, d).wait_recv()
        g4(k, 0).start()
        g4(k, 1).start()
        p4(k, 0).start()
        p4(k, 1).start()

    def collect_second(k):
        g4(k, 0).wait_recv()
        g4(k, 2).start()
        p4(k, 0).wait_recv()
        p4(k, 2).start()

    def measure(k):
        for stage in (1, 2):
            g4(k, stage).wait_recv()
        squares = 0.0
        for n in range(4):
            s = scaled[k, n]
            squares += jnp.sum((dot(gram[k, 0], s) + dot(gram[k, 1], s)) * s.astype(F32))
        sq_buf[0, k] = jnp.full(sq_buf.shape[2:], squares, F32)

    def make_gram():
        for k in range(2):
            upper, lower = split(dot_first(basis[k], basis[k]))
            gram[k, 0] = upper
            gram[k, 1] = lower

    jobs = {
        "begin": lambda k: s1(k).start(), "first": arrive_first, "inner": arrive_inner,
        "second": arrive_second, "third": arrive_third, "relay": relay, "halve": halve,
        "quarter": quarter, "update": update, "collect": collect, "again": collect_second,
        "measure": measure, "gram": make_gram,
    }
    acc[...] = jnp.zeros_like(acc)
    b_load(0).wait()

    def one_step(i, carry):
        k, c = i // CHUNKS, lax.rem(i, CHUNKS)

        @pl.when(k == 0)
        def _():
            x_load(c).wait()
            c_load(0, c).wait()

        @pl.when(k == 1)
        def _():
            c_load(1, c).wait()

        @pl.when(i == CHUNKS)
        def _():
            b_load(1).wait()

        for step in sorted({entry[0] for entry in EARLY}):
            @pl.when(i == step)
            def _():
                for entry in EARLY:
                    if entry[0] == step:
                        jobs[entry[1]](*entry[2:])

        upper, lower = split(
            lax.dot_general(basis[k], x_buf[c], (((0,), (1,)), ((), ())), preferred_element_type=F32)
        )
        for n in range(4):
            cot = cot_buf[k, c, :, n * width : (n + 1) * width]
            acc[k, n] += dot(upper, cot) + dot(lower, cot)
        return carry

    lax.fori_loop(0, 2 * CHUNKS, one_step, 0)
    for name, *where in LATE:
        jobs[name](*where)

    q4 = send(sq_buf.at[0], sq_buf.at[1], q_send, q_recv, tp=1 - t)
    q4.start()
    for k in range(2):
        for stage in (1, 2):
            p4(k, stage).wait_recv()
    for slot in (1, 2, 3):
        for c in range(4):
            if c not in RELAY_X:
                to_y(slot, c).wait_recv()
            else:
                relay_x(slot, c).wait_recv()
                relay_x(slot, c).wait_send()
            if c not in RELAY_Y:
                to_x(slot, c).wait_recv()
            else:
                relay_y(slot, c).wait_recv()
                relay_y(slot, c).wait_send()
            to_x(slot, c).wait_send()
            to_y(slot, c).wait_send()
    for i in range(count):
        own_ahead(i).wait_send()

        @pl.when(inner)
        def _():
            own_behind(i).wait_send()
            for slot in (1, 2, 3):
                pass_along(slot, i).wait_send()
    for k in range(2):
        s1(k).wait_send()
        s2(k).wait_send()
        for d in range(1, n_fs):
            s3(k, d).wait_send()
            a4(k, d).wait_send()
        for stage in range(3):
            g4(k, stage).wait_send()
            p4(k, stage).wait_send()
    for o in range(2 if EXTRA else 1, 4):
        for k in range(2):
            w_load(o, k).wait()
    q4.wait()
    squares_out[...] = sq_buf[0] + sq_buf[1]


def finish_block(
    entries, gathered, scaled, proj, squares, basis, weight, moments,
    value_new, gate_new, value_copy, gate_copy, value_step, gate_step,
    value_first_new, gate_first_new, value_second_new, gate_second_new,
    new_buf, step_buf, copy_buf, moment_buf, new_sem, step_sem, copy_sem, moment_sem,
):
    f = lax.axis_index("fs")
    rows = weight.shape[1]
    model = gathered.shape[1]
    width = scaled.shape[3]
    block = min(rows, 256)
    own = rows // block
    blocks = model // block
    news, copies, steps = (value_new, gate_new), (value_copy, gate_copy), (value_step, gate_step)
    factors = [lax.rsqrt(squares[k, :1, :1] / entries + 1e-06) for k in range(2)]

    def span(start, size):
        return pl.ds(pl.multiple_of(start, size), size)

    def row_of(b):
        return lax.rem(f * own + b, blocks) * block

    def new_out(k, b):
        return pltpu.make_async_copy(
            new_buf.at[k, span(b * block, block)], news[k].at[span(b * block, block)], new_sem.at[k, b])

    def step_store(k, b):
        return pltpu.make_async_copy(
            step_buf.at[k, span(b * block, block)], steps[k].at[span(b * block, block)], step_sem.at[k, b])

    def copy_out(k, b):
        where = span(row_of(b), block)
        return pltpu.make_async_copy(copy_buf.at[k, where], copies[k].at[where], copy_sem.at[k, b])

    def own_block(b, carry):
        for k in range(2):
            where = span(row_of(b), block)
            local_rows = span(b * block, block)
            for n in range(4):
                cols = slice(n * width, (n + 1) * width)
                direction = dot(basis[k, where], scaled[k, n]) * factors[k]
                updated = weight[k, local_rows, cols] - learn_rate * direction
                step_buf[k, local_rows, cols] = direction
                new_buf[k, local_rows, cols] = updated
                copy_buf[k, where, cols] = updated.astype(BF16)
            step_store(k, b).start()
            new_out(k, b).start()
            copy_out(k, b).start()
        return carry

    lax.fori_loop(0, own, own_block, 0)
    outs = (value_first_new, gate_first_new, value_second_new, gate_second_new)
    for k in range(2):
        for n in range(4):
            cols = slice(n * width, (n + 1) * width)
            small = proj[k, n].astype(F32)
            moment_buf[k, :, cols] = 0.9 * moments[k, :, cols] + 0.1 * small
            moment_buf[2 + k, :, cols] = 0.95 * moments[2 + k, :, cols] + 0.05 * small * small
    moment_outs = [pltpu.make_async_copy(moment_buf.at[i], outs[i], moment_sem.at[i]) for i in range(4)]
    for copy in moment_outs:
        copy.start()

    def other_block(b, carry):
        for k in range(2):
            where = span(row_of(b), block)
            for n in range(4):
                cols = slice(n * width, (n + 1) * width)
                direction = dot(basis[k, where], scaled[k, n]) * (learn_rate * factors[k])
                copy_buf[k, where, cols] = (gathered[k, where, cols].astype(F32) - direction).astype(BF16)
            copy_out(k, b).start()
        return carry

    lax.fori_loop(own, blocks, other_block, 0)

    def drain_own(b, carry):
        for k in range(2):
            step_store(k, b).wait()
            new_out(k, b).wait()
        return carry

    def drain(b, carry):
        for k in range(2):
            copy_out(k, b).wait()
        return carry

    lax.fori_loop(0, own, drain_own, 0)
    lax.fori_loop(0, blocks, drain, 0)
    for copy in moment_outs:
        copy.wait()


def local_block(*args):
    (mixer, value_cot, gate_cot, value_weight, gate_weight, value_basis, gate_basis,
     value_first, gate_first, value_second, gate_second) = args
    n_fs = 4
    tokens, model = mixer.shape
    half = value_cot.shape[1]
    rows = value_weight.shape[0]
    rank = value_basis.shape[1]
    low = value_first.shape[0]
    width = half // 4
    chunk = tokens // CHUNKS
    count = 4 + len(EXTRA)
    hbm = pl.BlockSpec(memory_space=pltpu.HBM)
    vmem = pl.BlockSpec(memory_space=pltpu.VMEM)
    dma = pltpu.SemaphoreType.DMA
    scratch = [
        pltpu.VMEM((CHUNKS, chunk, model), BF16),
        pltpu.VMEM((2, CHUNKS, chunk, half), BF16),
        pltpu.VMEM((2, 2, rank, rank), BF16),
        pltpu.VMEM((2, 4, rank, width), F32),
        pltpu.VMEM((2, 2, rank, width), F32),
        pltpu.VMEM((2, rank, width), F32),
        pltpu.VMEM((2, rank, width), F32),
        pltpu.VMEM((2, rank, width), F32),
        pltpu.VMEM((2, n_fs - 1, low, width), F32),
        pltpu.VMEM((2, 2, 8, 128), F32),
        dma((CHUNKS,)), dma((2, CHUNKS)), dma((2,)), dma((4, 2)), dma((4,)),
        dma((5, count)), dma((3, count)),
    ]
    scratch += [dma((3, 4)) for _ in range(8)]
    scratch += [dma((2,)) for _ in range(4)]
    scratch += [dma((2, 3)) for _ in range(8)]
    scratch += [dma(()), dma(())]
    outs = pl.pallas_call(
        exchange_block,
        out_shape=(
            pltpu.VMEM((2, model, half), BF16),
            pltpu.VMEM((2, 4, rank, width), BF16),
            pltpu.VMEM((2, 4, low, width), BF16),
            pltpu.VMEM((2, 8, 128), F32),
            pltpu.VMEM((2, model, rank), BF16),
            pltpu.VMEM((2, rows, half), F32),
            pltpu.VMEM((4, low, half), F32),
        ),
        in_specs=[hbm] * 11,
        out_specs=(vmem,) * 7,
        scratch_shapes=scratch,
        compiler_params=pltpu.CompilerParams(
            collective_id=0, has_side_effects=True, vmem_limit_bytes=VMEM_FIRST
        ),
        name="exchange_block",
    )(*args)
    outs = [pltpu.with_memory_space_constraint(out, pltpu.VMEM) for out in outs]
    block = min(rows, 256)
    return pl.pallas_call(
        functools.partial(finish_block, float(model) * half * 2),
        in_specs=[vmem] * 7,
        out_specs=[hbm] * 10,
        out_shape=[
            jax.ShapeDtypeStruct((rows, half), F32),
            jax.ShapeDtypeStruct((rows, half), F32),
            jax.ShapeDtypeStruct((model, half), BF16),
            jax.ShapeDtypeStruct((model, half), BF16),
            jax.ShapeDtypeStruct((rows, half), F32),
            jax.ShapeDtypeStruct((rows, half), F32),
        ] + [jax.ShapeDtypeStruct((low, half), F32)] * 4,
        scratch_shapes=[
            pltpu.VMEM((2, rows, half), F32),
            pltpu.VMEM((2, rows, half), F32),
            pltpu.VMEM((2, model, half), BF16),
            pltpu.VMEM((4, low, half), F32),
            dma((2, rows // block)), dma((2, rows // block)), dma((2, model // block)), dma((4,)),
        ],
        compiler_params=pltpu.CompilerParams(vmem_limit_bytes=VMEM_SECOND),
        name="finish_block",
    )(*outs)


def solution(mesh):
    sizes = tuple(mesh.shape[name] for name in ("fs", "rep", "tp"))
    return jax.shard_map(
        lambda *args: tuple(local_block(*args) if sizes == (4, 4, 2) else local(sizes, *args)),
        mesh=mesh,
        in_specs=(
            P(("fs", "rep"), None),
            P(("fs", "rep"), "tp"),
            P(("fs", "rep"), "tp"),
            P("fs", "tp"),
            P("fs", "tp"),
            P(),
            P(),
            P("fs", "tp"),
            P("fs", "tp"),
            P("fs", "tp"),
            P("fs", "tp"),
        ),
        out_specs=(
            P("fs", "tp"),
            P("fs", "tp"),
            P(None, "tp"),
            P(None, "tp"),
            P("fs", "tp"),
            P("fs", "tp"),
            P("fs", "tp"),
            P("fs", "tp"),
            P("fs", "tp"),
            P("fs", "tp"),
        ),
        check_vma=False,
    )
```

```python
import functools

import jax
import jax.numpy as jnp
from jax import lax
from jax.experimental import pallas as pl
from jax.experimental.pallas import tpu as pltpu
from jax.sharding import PartitionSpec as P

learn_rate = 0.02
CHUNKS = 4
VMEM_FIRST = 40 * 1024 * 1024
VMEM_SECOND = 40 * 1024 * 1024
F32 = jnp.float32
BF16 = jnp.bfloat16


def dot(a, b):
    return jnp.dot(a, b, preferred_element_type=F32)


def dot_first(a, b):
    return lax.dot_general(a, b, (((0,), (0,)), ((), ())), preferred_element_type=F32)


def split(a):
    upper = a.astype(BF16)
    return upper, (a - upper.astype(F32)).astype(BF16)


def exchange(
    n_fs, n_rep, n_tp,
    mixer, value_cot, gate_cot, value_weight, gate_weight, value_basis, gate_basis,
    value_first_hbm, gate_first_hbm, value_second_hbm, gate_second_hbm,
    value_rows, gate_rows, scaled_out, projected_out, squares_out,
    x_buf, cot_buf, w_buf, w_half, basis_buf, gram, acc, part_in,
    mid, mid_in, proj_all, scaled, sq_buf, moments,
    x_sem, w_sem, b_sem, own_sem, m_sem,
    w1_send, w1_recv, w2_send, w2_recv,
    s1_send, s1_recv, s2_send, s2_recv, p_send, p_recv, a_send, a_recv, g_send, g_recv, q_send, q_recv,
):
    f, r, t = lax.axis_index("fs"), lax.axis_index("rep"), lax.axis_index("tp")
    cots = (value_cot, gate_cot)
    weights = (value_weight, gate_weight)
    bases = (value_basis, gate_basis)
    gathered = (value_rows, gate_rows)
    tokens = mixer.shape[0]
    chunk = tokens // CHUNKS
    rows = value_weight.shape[0]
    share = rows // n_rep
    width = acc.shape[2]
    per_role = n_rep // 2
    low = mid.shape[1]

    def fs_at(d):
        return lax.rem(f + d, n_fs)

    def rep_at(d):
        return lax.rem(r + d, n_rep)

    def send(src, dst, s, v, **where):
        return pltpu.make_async_remote_copy(
            src_ref=src, dst_ref=dst, send_sem=s, recv_sem=v,
            device_id=where, device_id_type=pl.DeviceIdType.MESH,
        )

    w_loads = [pltpu.make_async_copy(weights[k], w_buf.at[k], w_sem.at[k]) for k in range(2)]
    b_loads = [pltpu.make_async_copy(bases[k], basis_buf.at[k], b_sem.at[k]) for k in range(2)]

    def x_loads(c):
        span = pl.ds(pl.multiple_of(c * chunk, chunk), chunk)
        return [pltpu.make_async_copy(mixer.at[span], x_buf.at[c], x_sem.at[c, 0])] + [
            pltpu.make_async_copy(cots[k].at[span], cot_buf.at[k, c], x_sem.at[c, 1 + k]) for k in range(2)
        ]

    m_loads = [
        pltpu.make_async_copy(ref, moments.at[i], m_sem.at[i])
        for i, ref in enumerate((value_first_hbm, gate_first_hbm, value_second_hbm, gate_second_hbm))
    ]
    for copy in w_loads + b_loads:
        copy.start()
    for c in range(CHUNKS):
        for copy in x_loads(c):
            copy.start()

    for copy in m_loads:
        copy.start()

    barrier = pltpu.get_barrier_semaphore()
    for d in range(1, n_fs):
        pl.semaphore_signal(barrier, inc=1, device_id={"fs": fs_at(d)}, device_id_type=pl.DeviceIdType.MESH)
    for d in range(1, n_rep):
        pl.semaphore_signal(barrier, inc=1, device_id={"rep": rep_at(d)}, device_id_type=pl.DeviceIdType.MESH)
    for d in range(1, n_tp):
        pl.semaphore_signal(
            barrier, inc=1, device_id={"tp": lax.rem(t + d, n_tp)}, device_id_type=pl.DeviceIdType.MESH
        )
    for k in range(2):
        w_loads[k].wait()
        w_half[k] = w_buf[k].astype(BF16)
    pl.semaphore_wait(barrier, n_fs + n_rep + n_tp - 3)

    def share_of(block, part_index):
        return pl.ds(pl.multiple_of(block * rows + part_index * share, share), share)

    w1 = {}
    for d in range(1, n_fs):
        for k in range(2):
            w1[d, k] = send(
                w_half.at[k, pl.ds(pl.multiple_of(r * share, share), share)],
                gathered[k].at[share_of(f, r)],
                w1_send.at[d - 1, k], w1_recv.at[d - 1, k], fs=fs_at(d),
            )
            w1[d, k].start()
    own = []
    for k in range(2):
        copy = pltpu.make_async_copy(
            w_half.at[k], gathered[k].at[pl.ds(pl.multiple_of(f * rows, rows), rows)], own_sem.at[k]
        )
        copy.start()
        own.append(copy)

    for copy in b_loads:
        copy.wait()
    acc[...] = jnp.zeros_like(acc)

    def one_chunk(c, carry):
        for copy in x_loads(c):
            copy.wait()
        x = x_buf[c]
        for k in range(2):
            upper, lower = split(dot(x, basis_buf[k]))
            for q in range(per_role):
                cols = slice(q * width, (q + 1) * width)
                cot = cot_buf[k, c, :, cols]
                acc[k * per_role + q] += dot_first(upper, cot) + dot_first(lower, cot)
        return carry

    lax.fori_loop(0, CHUNKS, one_chunk, 0)
    s1 = {}
    for d in range(1, n_rep):
        s1[d] = send(
            acc.at[rep_at(d)], part_in.at[d - 1], s1_send.at[d - 1], s1_recv.at[d - 1], rep=rep_at(d)
        )
        s1[d].start()

    w2, heard = {}, set()
    near, far = (r + 1 - 2 * lax.rem(r, 2), lax.rem(r + 2, n_rep)) if n_rep == 4 else (None, None)

    def pass_on(d, e, k, owner, peer):
        source = lax.rem(f - d + n_fs, n_fs)
        rows_ref = gathered[k].at[share_of(source, owner)]
        w2[d, e, k] = send(
            rows_ref, rows_ref, w2_send.at[d - 1, e, k], w2_recv.at[d - 1, e, k], rep=peer
        )
        w2[d, e, k].start()

    def forward(d):
        for k in range(2):
            w1[d, k].wait_recv()
            peers = (near, far) if n_rep == 4 else [rep_at(e) for e in range(1, n_rep)]
            for e, peer in enumerate(peers):
                pass_on(d, e, k, r, peer)

    def relay(d):
        if n_rep == 4:
            for e, k, owner, peer in ((0, 0, near, far), (1, 1, far, near)):
                w2[d, e, k].wait_recv()
                heard.add((d, e, k))
                pass_on(d, 2, k, owner, peer)

    forward(1)
    for k in range(2):
        upper, lower = split(dot_first(basis_buf[k], basis_buf[k]))
        gram[k, 0] = upper
        gram[k, 1] = lower

    for d in range(1, n_rep):
        s1[d].wait_recv()
    total = acc[r]
    for d in range(1, n_rep):
        total += part_in[d - 1]
    mid[...] = total.reshape(mid.shape)
    s2 = {}
    for d in range(1, n_fs):
        s2[d] = send(
            mid.at[fs_at(d)], mid_in.at[d - 1], s2_send.at[d - 1], s2_recv.at[d - 1], fs=fs_at(d)
        )
        s2[d].start()
    for d in range(2, n_fs - 1):
        forward(d)
        relay(d - 1)
    for d in range(1, n_fs):
        s2[d].wait_recv()
    small = mid[f]
    for d in range(1, n_fs):
        small += mid_in[d - 1]
    proj_all[r] = small.astype(BF16)

    cols = pl.ds(pl.multiple_of(lax.rem(r, per_role) * width, width), width)
    is_value = r < per_role
    for copy in m_loads:
        copy.wait()
    first = jnp.where(is_value, moments[0, :, cols], moments[1, :, cols])
    second = jnp.where(is_value, moments[2, :, cols], moments[3, :, cols])
    first_new = 0.9 * first + 0.1 * small
    second_new = 0.95 * second + 0.05 * small * small
    scaled[r, f] = (first_new * lax.rsqrt(second_new)).astype(BF16)
    a4, p4, g4 = {}, {}, {}
    for d in range(1, n_fs):
        a4[d] = send(
            scaled.at[r, f], scaled.at[r, f], a_send.at[d - 1], a_recv.at[d - 1], fs=fs_at(d)
        )
        a4[d].start()
    for d in range(1, n_rep):
        p4[d] = send(proj_all.at[r], proj_all.at[r], p_send.at[d - 1], p_recv.at[d - 1], rep=rep_at(d))
        p4[d].start()
    if n_fs > 2:
        forward(n_fs - 1)
        relay(n_fs - 2)
    for d in range(1, n_fs):
        a4[d].wait_recv()
    for d in range(1, n_rep):
        g4[d] = send(scaled.at[r], scaled.at[r], g_send.at[d - 1], g_recv.at[d - 1], rep=rep_at(d))
        g4[d].start()
    relay(n_fs - 1)
    for d in range(1, n_rep):
        g4[d].wait_recv()

    for k in range(2):
        squares = 0.0
        for q in range(per_role):
            s = scaled[k * per_role + q].reshape(n_fs * low, width)
            squares += jnp.sum((dot(gram[k, 0], s) + dot(gram[k, 1], s)) * s.astype(F32))
        sq_buf[0, k] = jnp.full(sq_buf.shape[2:], squares, F32)
    q4 = []
    for d in range(1, n_tp):
        copy = send(
            sq_buf.at[0], sq_buf.at[d], q_send.at[d - 1], q_recv.at[d - 1], tp=lax.rem(t + d, n_tp)
        )
        copy.start()
        q4.append(copy)
    for d in range(1, n_rep):
        p4[d].wait_recv()
    scaled_out[...] = scaled[...].reshape(scaled_out.shape)
    projected_out[...] = proj_all[...]
    for copy in q4:
        copy.wait_recv()
    sums = sq_buf[0]
    for d in range(1, n_tp):
        sums += sq_buf[d]
    squares_out[...] = sums

    for copy in list(w1.values()) + list(s1.values()) + list(s2.values()) + list(a4.values()):
        copy.wait_send()
    for copy in list(p4.values()) + list(g4.values()) + q4:
        copy.wait_send()
    for copy in own:
        copy.wait()
    for key, copy in w2.items():
        copy.wait_send()
        if key not in heard:
            copy.wait_recv()


def finish(
    own_blocks, entries,
    where, value_rows, gate_rows, value_basis, gate_basis, value_weight, gate_weight,
    scaled, projected, squares, value_first, gate_first, value_second, gate_second,
    value_new, gate_new, value_copy, gate_copy, value_step, gate_step,
    value_first_new, gate_first_new, value_second_new, gate_second_new,
):
    step = pl.program_id(0)
    width = scaled.shape[2]
    per_role = scaled.shape[0] // 2
    roles = (
        (value_rows, value_basis, value_weight, value_new, value_copy, value_step),
        (gate_rows, gate_basis, gate_weight, gate_new, gate_copy, gate_step),
    )
    for k, (rows, basis, weight, new, copy, step_out) in enumerate(roles):
        factor = lax.rsqrt(squares[k, :1, :1] / entries + 1e-06)
        for q in range(per_role):
            cols = slice(q * width, (q + 1) * width)
            direction = dot(basis[...], scaled[k * per_role + q]) * factor
            copy[:, cols] = (rows[:, cols].astype(F32) - learn_rate * direction).astype(BF16)

            @pl.when(step < own_blocks)
            def _():
                step_out[:, cols] = direction
                new[:, cols] = weight[:, cols] - learn_rate * direction

    @pl.when(step == 0)
    def _():
        moments = (
            (value_first, value_second, value_first_new, value_second_new),
            (gate_first, gate_second, gate_first_new, gate_second_new),
        )
        for k, (first, second, first_new, second_new) in enumerate(moments):
            for q in range(per_role):
                cols = slice(q * width, (q + 1) * width)
                small = projected[k * per_role + q].astype(F32)
                first_new[:, cols] = 0.9 * first[:, cols] + 0.1 * small
                second_new[:, cols] = 0.95 * second[:, cols] + 0.05 * small * small


def local(sizes, *args):
    n_fs, n_rep, n_tp = sizes
    (mixer, value_cot, gate_cot, value_weight, gate_weight, value_basis, gate_basis,
     value_first, gate_first, value_second, gate_second) = args
    tokens, model = mixer.shape
    half = value_cot.shape[1]
    rows = value_weight.shape[0]
    rank = value_basis.shape[1]
    low = value_first.shape[0]
    width = 2 * half // n_rep
    chunk = tokens // CHUNKS
    any_spec = pl.BlockSpec(memory_space=pl.ANY)
    vmem = pl.BlockSpec(memory_space=pltpu.VMEM)
    dma = pltpu.SemaphoreType.DMA
    scratch = [
        pltpu.VMEM((CHUNKS, chunk, model), BF16),
        pltpu.VMEM((2, CHUNKS, chunk, half), BF16),
        pltpu.VMEM((2, rows, half), F32),
        pltpu.VMEM((2, rows, half), BF16),
        pltpu.VMEM((2, model, rank), BF16),
        pltpu.VMEM((2, 2, rank, rank), BF16),
        pltpu.VMEM((n_rep, rank, width), F32),
        pltpu.VMEM((n_rep - 1, rank, width), F32),
        pltpu.VMEM((n_fs, low, width), F32),
        pltpu.VMEM((n_fs - 1, low, width), F32),
        pltpu.VMEM((n_rep, low, width), BF16),
        pltpu.VMEM((n_rep, n_fs, low, width), BF16),
        pltpu.VMEM((n_tp, 2, 8, 128), F32),
        pltpu.VMEM((4, low, half), F32),
        dma((CHUNKS, 3)), dma((2,)), dma((2,)), dma((2,)), dma((4,)),
        dma((n_fs - 1, 2)), dma((n_fs - 1, 2)),
        dma((n_fs - 1, n_rep - 1, 2)), dma((n_fs - 1, n_rep - 1, 2)),
    ]
    for count in (n_rep, n_fs, n_rep, n_fs, n_rep, n_tp):
        scratch += [dma((count - 1,)), dma((count - 1,))]
    value_rows, gate_rows, scaled, projected, squares = pl.pallas_call(
        functools.partial(exchange, n_fs, n_rep, n_tp),
        out_shape=(
            jax.ShapeDtypeStruct((rows * n_fs, half), BF16),
            jax.ShapeDtypeStruct((rows * n_fs, half), BF16),
            jax.ShapeDtypeStruct((n_rep, rank, width), BF16),
            jax.ShapeDtypeStruct((n_rep, low, width), BF16),
            jax.ShapeDtypeStruct((2, 8, 128), F32),
        ),
        in_specs=[any_spec] * 11,
        out_specs=(any_spec, any_spec, vmem, vmem, vmem),
        scratch_shapes=scratch,
        compiler_params=pltpu.CompilerParams(
            collective_id=0, has_side_effects=True, vmem_limit_bytes=52 * 1024 * 1024
        ),
        name="exchange",
    )(*args)

    block = min(rows, 256)
    own_blocks = rows // block
    blocks = model // block
    where = (lax.axis_index("fs") * own_blocks).astype(jnp.int32).reshape(1)

    def turned(i, w):
        return (lax.rem(w[0] + i, blocks), 0)

    def own(i, w):
        return (jnp.minimum(i, own_blocks - 1), 0)

    def whole(shape):
        return pl.BlockSpec(shape, lambda i, w: (0,) * len(shape))

    row_spec = pl.BlockSpec((block, half), turned)
    basis_spec = pl.BlockSpec((block, rank), turned)
    own_spec = pl.BlockSpec((block, half), own)
    moment = whole((low, half))
    return pl.pallas_call(
        functools.partial(finish, own_blocks, float(model) * half * n_tp),
        grid_spec=pltpu.PrefetchScalarGridSpec(
            num_scalar_prefetch=1,
            grid=(blocks,),
            in_specs=[row_spec, row_spec, basis_spec, basis_spec, own_spec, own_spec,
                      whole(scaled.shape), whole(projected.shape), whole(squares.shape)] + [moment] * 4,
            out_specs=[own_spec, own_spec, row_spec, row_spec, own_spec, own_spec] + [moment] * 4,
        ),
        out_shape=[
            jax.ShapeDtypeStruct((rows, half), F32),
            jax.ShapeDtypeStruct((rows, half), F32),
            jax.ShapeDtypeStruct((model, half), BF16),
            jax.ShapeDtypeStruct((model, half), BF16),
            jax.ShapeDtypeStruct((rows, half), F32),
            jax.ShapeDtypeStruct((rows, half), F32),
        ] + [jax.ShapeDtypeStruct((low, half), F32)] * 4,
        compiler_params=pltpu.CompilerParams(vmem_limit_bytes=40 * 1024 * 1024),
        name="finish",
    )(where, value_rows, gate_rows, value_basis, gate_basis, value_weight, gate_weight,
      scaled, projected, squares, value_first, gate_first, value_second, gate_second)


PIECES = 8
EXTRA = (0, 1, 2, 3, 4)
RELAY_X = ((5, 6), (5,), (5, 6))
RELAY_Y = ((7,), (6, 7), (7,))
EARLY = (
    (0, "open"), (2, "first", 0), (3, "first", 1), (4, "inner", 0), (4, "inner", 1), (4, "first", 2),
    (6, "first", 3), (6, "first", 4), (6, "begin", 0, 0), (6, "inner", 4), (9, "begin", 0, 1),
    (9, "first", 5), (9, "inner", 5), (9, "first", 6), (13, "begin", 1, 0), (13, "halve", 0),
    (13, "inner", 9), (14, "relay", 1, 6), (14, "begin", 1, 1), (14, "inner", 2), (14, "inner", 6),
    (14, "inner", 7), (15, "halve", 1), (15, "second", 2), (15, "inner", 8), (15, "inner", 12),
    (15, "first", 7), (15, "inner", 3), (15, "second", 7), (15, "third", 2), (15, "second", 0),
    (15, "quarter", 0), (15, "gram"), (15, "second", 5), (15, "third", 7), (15, "second", 6),
    (15, "inner", 10), (15, "third", 0), (15, "second", 1),
)
LATE = (
    ("relay", 1, 5), ("quarter", 1), ("second", 4), ("update", 0), ("first", 10), ("third", 5), ("third", 6),
    ("relay", 3, 7), ("third", 1), ("first", 8), ("update", 1), ("second", 3), ("third", 4), ("collect", 0),
    ("collect", 1), ("first", 9), ("inner", 11), ("first", 12), ("second", 10), ("relay", 3, 6), ("again", 0),
    ("relay", 3, 5), ("third", 3), ("first", 11), ("relay", 2, 6), ("third", 10), ("second", 11),
    ("second", 12), ("relay", 2, 5), ("again", 1), ("relay", 1, 7), ("third", 11), ("relay", 2, 7),
    ("second", 9), ("second", 8), ("third", 9), ("third", 8), ("measure", 1), ("third", 12), ("measure", 0),
)


def exchange_block(
    mixer, value_cot, gate_cot, value_weight, gate_weight, value_basis, gate_basis,
    value_first, gate_first, value_second, gate_second,
    gathered, scaled, proj, squares_out, basis, weight, moments,
    x_buf, cot_buf, gram, turned, acc, first_in, second_out, second_in, part, part_in, sq_buf,
    x_sem, c_sem, b_sem, w_sem, m_sem,
    z_send, z_recv, x_send, x_recv, y_send, y_recv, rx_send, rx_recv, ry_send, ry_recv,
    s1_send, s1_recv, s2_send, s2_recv, s3_send, s3_recv, a_send, a_recv,
    g_send, g_recv, p_send, p_recv, q_send, q_recv,
):
    f, r, t = lax.axis_index("fs"), lax.axis_index("rep"), lax.axis_index("tp")
    n_fs = 4
    cots = (value_cot, gate_cot)
    weights = (value_weight, gate_weight)
    bases = (value_basis, gate_basis)
    tokens = mixer.shape[0]
    chunk = tokens // CHUNKS
    rows = value_weight.shape[0]
    share = rows // 4
    piece_rows = 2 * share // PIECES
    low = moments.shape[1]
    width = acc.shape[3]
    ends = jnp.logical_or(f == 0, f == n_fs - 1)
    inner = jnp.logical_not(ends)
    turn = 1 - 2 * (f // 2)
    ahead = f + turn
    behind = jnp.clip(f - turn, 0, n_fs - 1)
    x_at, y_at = lax.rem(r, 2), r // 2
    x_peer, y_peer = r + 1 - 2 * x_at, r + 2 - 4 * y_at
    across = 3 - r
    half_at, part_at = (x_at, y_at), (y_at, x_at)
    half_peer, part_peer = (x_peer, y_peer), (y_peer, x_peer)
    mine = [2 * half_at[k] + part_at[k] for k in range(2)]

    def fs_at(d):
        return lax.rem(f + d, n_fs)

    def send(src, dst, s, v, **where):
        return pltpu.make_async_remote_copy(
            src_ref=src, dst_ref=dst, send_sem=s, recv_sem=v,
            device_id=where, device_id_type=pl.DeviceIdType.MESH,
        )

    def span(start, size):
        return pl.ds(pl.multiple_of(start, size), size)

    def piece(plane, quarter, c):
        return gathered.at[c % 2, span(plane * rows + quarter * share + (c // 2) * piece_rows, piece_rows)]

    z_pieces = [(r, c) for c in range(PIECES)] + [(across, c) for c in EXTRA]
    count = len(z_pieces)
    order = (r, across, x_peer, y_peer)

    def w_load(o, k):
        where = span(order[o] * share, share)
        return pltpu.make_async_copy(weights[k].at[where], weight.at[k, where], w_sem.at[o, k])

    def b_load(k):
        return pltpu.make_async_copy(bases[k], basis.at[k], b_sem.at[k])

    def x_load(c):
        return pltpu.make_async_copy(mixer.at[span(c * chunk, chunk)], x_buf.at[c], x_sem.at[c])

    def c_load(k):
        return pltpu.make_async_copy(cots[k], cot_buf.at[k], c_sem.at[k])

    m_loads = [
        pltpu.make_async_copy(ref, moments.at[i], m_sem.at[i])
        for i, ref in enumerate((value_first, gate_first, value_second, gate_second))
    ]
    b_load(0).start()
    x_load(0).start()
    for o in range(2 if EXTRA else 1):
        for k in range(2):
            w_load(o, k).start()
    for c in range(1, CHUNKS):
        x_load(c).start()
    c_load(0).start()
    b_load(1).start()
    c_load(1).start()
    for copy in m_loads:
        copy.start()
    for o in range(2 if EXTRA else 1, 4):
        for k in range(2):
            w_load(o, k).start()

    barrier = pltpu.get_barrier_semaphore()
    for d in range(1, n_fs):
        pl.semaphore_signal(barrier, inc=1, device_id={"fs": fs_at(d)}, device_id_type=pl.DeviceIdType.MESH)
    for peer in (x_peer, y_peer):
        pl.semaphore_signal(barrier, inc=1, device_id={"rep": peer}, device_id_type=pl.DeviceIdType.MESH)
    pl.semaphore_signal(barrier, inc=1, device_id={"tp": 1 - t}, device_id_type=pl.DeviceIdType.MESH)

    def plane_of(slot):
        return lax.rem(f + turn * slot + n_fs, n_fs)

    landing = jnp.where(ends, 2, 0)

    def own_ahead(i):
        quarter, c = z_pieces[i]
        ref = piece(f, quarter, c)
        return send(ref, ref, z_send.at[0, i], z_recv.at[landing, i], fs=ahead)

    def own_behind(i):
        quarter, c = z_pieces[i]
        ref = piece(f, quarter, c)
        return send(ref, ref, z_send.at[1, i], z_recv.at[0, i], fs=behind)

    def pass_along(slot, i):
        quarter, c = z_pieces[i]
        ref = piece(plane_of(slot), quarter, c)
        if slot == 3:
            return send(ref, ref, z_send.at[4, i], z_recv.at[1, i], fs=ahead)
        return send(ref, ref, z_send.at[1 + slot, i], z_recv.at[slot, i], fs=behind)

    def arrival(slot, i):
        quarter, c = z_pieces[i]
        ref = piece(plane_of(slot), quarter, c)
        return send(ref, ref, z_send.at[0, i], z_recv.at[slot - 1, i], fs=ahead)

    def opening():
        for o in range(2 if EXTRA else 1):
            where = span(order[o] * share, share)
            for k in range(2):
                w_load(o, k).wait()
                gathered[k, span(f * rows + order[o] * share, share)] = weight[k, where].astype(BF16)
        pl.semaphore_wait(barrier, n_fs + 2)
        for i in range(count):
            own_ahead(i).start()

            @pl.when(inner)
            def _():
                own_behind(i).start()

    def to_x(slot, c):
        ref = piece(plane_of(slot), r, c)
        return send(ref, ref, x_send.at[slot - 1, c], x_recv.at[slot - 1, c], rep=x_peer)

    def to_y(slot, c):
        ref = piece(plane_of(slot), r, c)
        return send(ref, ref, y_send.at[slot - 1, c], y_recv.at[slot - 1, c], rep=y_peer)

    def relay_x(slot, c):
        ref = piece(plane_of(slot), y_peer, c)
        return send(ref, ref, rx_send.at[slot - 1, c], rx_recv.at[slot - 1, c], rep=x_peer)

    def relay_y(slot, c):
        ref = piece(plane_of(slot), x_peer, c)
        return send(ref, ref, ry_send.at[slot - 1, c], ry_recv.at[slot - 1, c], rep=y_peer)

    def spread(slot, i):
        if i < PIECES:
            to_x(slot, i).start()
            to_y(slot, i).start()

    def arrive_first(i):
        arrival(1, i).wait_recv()

        @pl.when(inner)
        def _():
            pass_along(1, i).start()

        spread(1, i)

    def arrive_inner(i):
        @pl.when(inner)
        def _():
            arrival(3, i).wait_recv()
            pass_along(3, i).start()

    def arrive_second(i):
        arrival(2, i).wait_recv()

        @pl.when(inner)
        def _():
            pass_along(2, i).start()

        spread(2, i)

    def arrive_third(i):
        @pl.when(ends)
        def _():
            arrival(3, i).wait_recv()

        spread(3, i)

    def relay(slot, c):
        if c in RELAY_X[slot - 1]:
            to_y(slot, c).wait_recv()
            relay_x(slot, c).start()
        if c in RELAY_Y[slot - 1]:
            to_x(slot, c).wait_recv()
            relay_y(slot, c).start()

    def s1(k, j):
        other = acc.at[k, 2 * (1 - half_at[k]) + (part_at[k] if j else 1 - part_at[k])]
        return send(other, first_in.at[k, j], s1_send.at[k, j], s1_recv.at[k, j], rep=half_peer[k])

    def s2(k):
        return send(second_out.at[k], second_in.at[k], s2_send.at[k], s2_recv.at[k], rep=part_peer[k])

    def s3(k, d):
        return send(
            part.at[k, span(fs_at(d) * low, low)], part_in.at[k, d - 1],
            s3_send.at[k, d - 1], s3_recv.at[k, d - 1], fs=fs_at(d),
        )

    def halve(k):
        s1(k, 0).wait_recv()
        second_out[k] = acc[k, 2 * half_at[k] + 1 - part_at[k]] + first_in[k, 0]
        s2(k).start()

    def quarter(k):
        s1(k, 1).wait_recv()
        s2(k).wait_recv()
        part[k] = acc[k, mine[k]] + first_in[k, 1] + second_in[k]
        for d in range(1, n_fs):
            s3(k, d).start()

    def a4(k, d):
        ref = scaled.at[k, mine[k], span(f * low, low)]
        return send(ref, ref, a_send.at[k, d - 1], a_recv.at[k, d - 1], fs=fs_at(d))

    def grow(buf, ss, vs, k, stage):
        if stage == 0:
            ref = buf.at[k, mine[k]]
            return send(ref, ref, ss.at[k, 0], vs.at[k, 0], rep=part_peer[k])
        if stage == 1:
            ref = buf.at[k, mine[k]]
            return send(ref, ref, ss.at[k, 1], vs.at[k, 1], rep=half_peer[k])
        ref = buf.at[k, 2 * half_at[k] + 1 - part_at[k]]
        return send(ref, ref, ss.at[k, 2], vs.at[k, 2], rep=half_peer[k])

    def g4(k, stage):
        return grow(scaled, g_send, g_recv, k, stage)

    def p4(k, stage):
        return grow(proj, p_send, p_recv, k, stage)

    def update(k):
        if k == 0:
            for copy in m_loads:
                copy.wait()
        for d in range(1, n_fs):
            s3(k, d).wait_recv()
        small = part[k, span(f * low, low)]
        for d in range(1, n_fs):
            small += part_in[k, d - 1]
        proj[k, mine[k]] = small.astype(BF16)
        cols = span(mine[k] * width, width)
        first_new = 0.9 * moments[k, :, cols] + 0.1 * small
        second_new = 0.95 * moments[2 + k, :, cols] + 0.05 * small * small
        scaled[k, mine[k], span(f * low, low)] = (first_new * lax.rsqrt(second_new)).astype(BF16)
        for d in range(1, n_fs):
            a4(k, d).start()

    def collect(k):
        for d in range(1, n_fs):
            a4(k, d).wait_recv()
        g4(k, 0).start()
        g4(k, 1).start()
        p4(k, 0).start()
        p4(k, 1).start()

    def collect_second(k):
        g4(k, 0).wait_recv()
        g4(k, 2).start()
        p4(k, 0).wait_recv()
        p4(k, 2).start()

    def measure(k):
        for stage in (1, 2):
            g4(k, stage).wait_recv()
        squares = 0.0
        for n in range(4):
            s = scaled[k, n]
            squares += jnp.sum((dot(gram[k, 0], s) + dot(gram[k, 1], s)) * s.astype(F32))
        sq_buf[0, k] = jnp.full(sq_buf.shape[2:], squares, F32)

    def make_gram():
        for k in range(2):
            upper, lower = split(dot_first(basis[k], basis[k]))
            gram[k, 0] = upper
            gram[k, 1] = lower

    jobs = {
        "open": opening, "begin": lambda k, j: s1(k, j).start(), "first": arrive_first, "inner": arrive_inner,
        "second": arrive_second, "third": arrive_third, "relay": relay, "halve": halve,
        "quarter": quarter, "update": update, "collect": collect, "again": collect_second,
        "measure": measure, "gram": make_gram,
    }
    rank = basis.shape[2]

    def one_step(i, carry):
        k, at = i // (CHUNKS + 4), lax.rem(i, CHUNKS + 4)
        for first in sorted({entry[0] for entry in EARLY}):
            @pl.when(i == first)
            def _():
                for entry in EARLY:
                    if entry[0] == first:
                        jobs[entry[1]](*entry[2:])

        for role in range(2):
            @pl.when(i == role * (CHUNKS + 4))
            def _():
                b_load(role).wait()

            @pl.when(i == role * (CHUNKS + 4) + CHUNKS)
            def _():
                c_load(role).wait()

        @pl.when(i < CHUNKS)
        def _():
            x_load(at).wait()

        @pl.when(at < CHUNKS)
        def _():
            upper, lower = split(
                lax.dot_general(basis[k], x_buf[at], (((0,), (1,)), ((), ())), preferred_element_type=F32)
            )
            turned[:rank, span(at * chunk, chunk)] = upper
            turned[rank:, span(at * chunk, chunk)] = lower

        @pl.when(at >= CHUNKS)
        def _():
            j = at - CHUNKS
            half_on, part_on = jnp.where(k == 0, x_at, y_at), jnp.where(k == 0, y_at, x_at)
            half_now = jnp.where(j < 2, 1 - half_on, half_on)
            part_now = jnp.where(lax.rem(j, 2) == 0, 1 - part_on, part_on)
            n = 2 * half_now + part_now
            cot = cot_buf[k, :, span(n * width, width)]
            acc[k, n] = dot(turned[:rank], cot) + dot(turned[rank:], cot)

        return carry

    lax.fori_loop(0, 2 * (CHUNKS + 4), one_step, 0)
    for name, *where in LATE:
        jobs[name](*where)

    q4 = send(sq_buf.at[0], sq_buf.at[1], q_send, q_recv, tp=1 - t)
    q4.start()
    for k in range(2):
        for stage in (1, 2):
            p4(k, stage).wait_recv()
    for slot in (1, 2, 3):
        for c in range(PIECES):
            if c not in RELAY_X[slot - 1]:
                to_y(slot, c).wait_recv()
            else:
                relay_x(slot, c).wait_recv()
                relay_x(slot, c).wait_send()
            if c not in RELAY_Y[slot - 1]:
                to_x(slot, c).wait_recv()
            else:
                relay_y(slot, c).wait_recv()
                relay_y(slot, c).wait_send()
            to_x(slot, c).wait_send()
            to_y(slot, c).wait_send()
    for i in range(count):
        own_ahead(i).wait_send()

        @pl.when(inner)
        def _():
            own_behind(i).wait_send()
            for slot in (1, 2, 3):
                pass_along(slot, i).wait_send()
    for k in range(2):
        s1(k, 0).wait_send()
        s1(k, 1).wait_send()
        s2(k).wait_send()
        for d in range(1, n_fs):
            s3(k, d).wait_send()
            a4(k, d).wait_send()
        for stage in range(3):
            g4(k, stage).wait_send()
            p4(k, stage).wait_send()
    for o in range(2 if EXTRA else 1, 4):
        for k in range(2):
            w_load(o, k).wait()
    q4.wait()
    squares_out[...] = sq_buf[0] + sq_buf[1]


def finish_block(
    entries, gathered, scaled, proj, squares, basis, weight, moments,
    value_new, gate_new, value_copy, gate_copy, value_step, gate_step,
    value_first_new, gate_first_new, value_second_new, gate_second_new,
    new_buf, step_buf, copy_buf, moment_buf, new_sem, step_sem, copy_sem, moment_sem,
):
    f = lax.axis_index("fs")
    rows = weight.shape[1]
    model = gathered.shape[1]
    width = scaled.shape[3]
    block = min(rows, 256)
    own = rows // block
    blocks = model // block
    news, copies, steps = (value_new, gate_new), (value_copy, gate_copy), (value_step, gate_step)
    factors = [lax.rsqrt(squares[k, :1, :1] / entries + 1e-06) for k in range(2)]

    def span(start, size):
        return pl.ds(pl.multiple_of(start, size), size)

    def row_of(b):
        return lax.rem(f * own + b, blocks) * block

    def new_out(k, b):
        return pltpu.make_async_copy(
            new_buf.at[k, span(b * block, block)], news[k].at[span(b * block, block)], new_sem.at[k, b])

    def step_store(k, b):
        return pltpu.make_async_copy(
            step_buf.at[k, span(b * block, block)], steps[k].at[span(b * block, block)], step_sem.at[k, b])

    def copy_out(k, b):
        where = span(row_of(b), block)
        return pltpu.make_async_copy(copy_buf.at[k, where], copies[k].at[where], copy_sem.at[k, b])

    def own_block(b, carry):
        for k in range(2):
            where = span(row_of(b), block)
            local_rows = span(b * block, block)
            for n in range(4):
                cols = slice(n * width, (n + 1) * width)
                direction = dot(basis[k, where], scaled[k, n]) * factors[k]
                updated = weight[k, local_rows, cols] - learn_rate * direction
                step_buf[k, local_rows, cols] = direction
                new_buf[k, local_rows, cols] = updated
                copy_buf[k, where, cols] = updated.astype(BF16)
            step_store(k, b).start()
            new_out(k, b).start()
            copy_out(k, b).start()
        return carry

    lax.fori_loop(0, own, own_block, 0)
    outs = (value_first_new, gate_first_new, value_second_new, gate_second_new)
    for k in range(2):
        for n in range(4):
            cols = slice(n * width, (n + 1) * width)
            small = proj[k, n].astype(F32)
            moment_buf[k, :, cols] = 0.9 * moments[k, :, cols] + 0.1 * small
            moment_buf[2 + k, :, cols] = 0.95 * moments[2 + k, :, cols] + 0.05 * small * small
    moment_outs = [pltpu.make_async_copy(moment_buf.at[i], outs[i], moment_sem.at[i]) for i in range(4)]
    for copy in moment_outs:
        copy.start()

    def other_block(b, carry):
        for k in range(2):
            where = span(row_of(b), block)
            for n in range(4):
                cols = slice(n * width, (n + 1) * width)
                direction = dot(basis[k, where], scaled[k, n]) * (learn_rate * factors[k])
                copy_buf[k, where, cols] = (gathered[k, where, cols].astype(F32) - direction).astype(BF16)
            copy_out(k, b).start()
        return carry

    lax.fori_loop(own, blocks, other_block, 0)

    def drain_own(b, carry):
        for k in range(2):
            step_store(k, b).wait()
            new_out(k, b).wait()
        return carry

    def drain(b, carry):
        for k in range(2):
            copy_out(k, b).wait()
        return carry

    lax.fori_loop(0, own, drain_own, 0)
    lax.fori_loop(0, blocks, drain, 0)
    for copy in moment_outs:
        copy.wait()


def local_block(*args):
    (mixer, value_cot, gate_cot, value_weight, gate_weight, value_basis, gate_basis,
     value_first, gate_first, value_second, gate_second) = args
    n_fs = 4
    tokens, model = mixer.shape
    half = value_cot.shape[1]
    rows = value_weight.shape[0]
    rank = value_basis.shape[1]
    low = value_first.shape[0]
    width = half // 4
    chunk = tokens // CHUNKS
    count = PIECES + len(EXTRA)
    hbm = pl.BlockSpec(memory_space=pltpu.HBM)
    vmem = pl.BlockSpec(memory_space=pltpu.VMEM)
    dma = pltpu.SemaphoreType.DMA
    scratch = [
        pltpu.VMEM((CHUNKS, chunk, model), BF16),
        pltpu.VMEM((2, tokens, half), BF16),
        pltpu.VMEM((2, 2, rank, rank), BF16),
        pltpu.VMEM((2 * rank, tokens), BF16),
        pltpu.VMEM((2, 4, rank, width), F32),
        pltpu.VMEM((2, 2, rank, width), F32),
        pltpu.VMEM((2, rank, width), F32),
        pltpu.VMEM((2, rank, width), F32),
        pltpu.VMEM((2, rank, width), F32),
        pltpu.VMEM((2, n_fs - 1, low, width), F32),
        pltpu.VMEM((2, 2, 8, 128), F32),
        dma((CHUNKS,)), dma((2,)), dma((2,)), dma((4, 2)), dma((4,)),
        dma((5, count)), dma((3, count)),
    ]
    scratch += [dma((3, PIECES)) for _ in range(8)]
    scratch += [dma((2, 2)), dma((2, 2)), dma((2,)), dma((2,))]
    scratch += [dma((2, 3)) for _ in range(8)]
    scratch += [dma(()), dma(())]
    outs = pl.pallas_call(
        exchange_block,
        out_shape=(
            pltpu.VMEM((2, model, half), BF16),
            pltpu.VMEM((2, 4, rank, width), BF16),
            pltpu.VMEM((2, 4, low, width), BF16),
            pltpu.VMEM((2, 8, 128), F32),
            pltpu.VMEM((2, model, rank), BF16),
            pltpu.VMEM((2, rows, half), F32),
            pltpu.VMEM((4, low, half), F32),
        ),
        in_specs=[hbm] * 11,
        out_specs=(vmem,) * 7,
        scratch_shapes=scratch,
        compiler_params=pltpu.CompilerParams(
            collective_id=0, has_side_effects=True, vmem_limit_bytes=VMEM_FIRST
        ),
        name="exchange_block",
    )(*args)
    outs = [pltpu.with_memory_space_constraint(out, pltpu.VMEM) for out in outs]
    block = min(rows, 256)
    return pl.pallas_call(
        functools.partial(finish_block, float(model) * half * 2),
        in_specs=[vmem] * 7,
        out_specs=[hbm] * 10,
        out_shape=[
            jax.ShapeDtypeStruct((rows, half), F32),
            jax.ShapeDtypeStruct((rows, half), F32),
            jax.ShapeDtypeStruct((model, half), BF16),
            jax.ShapeDtypeStruct((model, half), BF16),
            jax.ShapeDtypeStruct((rows, half), F32),
            jax.ShapeDtypeStruct((rows, half), F32),
        ] + [jax.ShapeDtypeStruct((low, half), F32)] * 4,
        scratch_shapes=[
            pltpu.VMEM((2, rows, half), F32),
            pltpu.VMEM((2, rows, half), F32),
            pltpu.VMEM((2, model, half), BF16),
            pltpu.VMEM((4, low, half), F32),
            dma((2, rows // block)), dma((2, rows // block)), dma((2, model // block)), dma((4,)),
        ],
        compiler_params=pltpu.CompilerParams(vmem_limit_bytes=VMEM_SECOND),
        name="finish_block",
    )(*outs)


def solution(mesh):
    sizes = tuple(mesh.shape[name] for name in ("fs", "rep", "tp"))
    return jax.shard_map(
        lambda *args: tuple(local_block(*args) if sizes == (4, 4, 2) else local(sizes, *args)),
        mesh=mesh,
        in_specs=(
            P(("fs", "rep"), None),
            P(("fs", "rep"), "tp"),
            P(("fs", "rep"), "tp"),
            P("fs", "tp"),
            P("fs", "tp"),
            P(),
            P(),
            P("fs", "tp"),
            P("fs", "tp"),
            P("fs", "tp"),
            P("fs", "tp"),
        ),
        out_specs=(
            P("fs", "tp"),
            P("fs", "tp"),
            P(None, "tp"),
            P(None, "tp"),
            P("fs", "tp"),
            P("fs", "tp"),
            P("fs", "tp"),
            P("fs", "tp"),
            P("fs", "tp"),
            P("fs", "tp"),
        ),
        check_vma=False,
    )
```

```python
import functools

import jax
import jax.numpy as jnp
from jax import lax
from jax.experimental import pallas as pl
from jax.experimental.pallas import tpu as pltpu
from jax.sharding import PartitionSpec as P

learn_rate = 0.02
CHUNKS = 4
VMEM_FIRST = 40 * 1024 * 1024
VMEM_SECOND = 40 * 1024 * 1024
F32 = jnp.float32
BF16 = jnp.bfloat16


def dot(a, b):
    return jnp.dot(a, b, preferred_element_type=F32)


def dot_first(a, b):
    return lax.dot_general(a, b, (((0,), (0,)), ((), ())), preferred_element_type=F32)


def split(a):
    upper = a.astype(BF16)
    return upper, (a - upper.astype(F32)).astype(BF16)


def exchange(
    n_fs, n_rep, n_tp,
    mixer, value_cot, gate_cot, value_weight, gate_weight, value_basis, gate_basis,
    value_first_hbm, gate_first_hbm, value_second_hbm, gate_second_hbm,
    value_rows, gate_rows, scaled_out, projected_out, squares_out,
    x_buf, cot_buf, w_buf, w_half, basis_buf, gram, acc, part_in,
    mid, mid_in, proj_all, scaled, sq_buf, moments,
    x_sem, w_sem, b_sem, own_sem, m_sem,
    w1_send, w1_recv, w2_send, w2_recv,
    s1_send, s1_recv, s2_send, s2_recv, p_send, p_recv, a_send, a_recv, g_send, g_recv, q_send, q_recv,
):
    f, r, t = lax.axis_index("fs"), lax.axis_index("rep"), lax.axis_index("tp")
    cots = (value_cot, gate_cot)
    weights = (value_weight, gate_weight)
    bases = (value_basis, gate_basis)
    gathered = (value_rows, gate_rows)
    tokens = mixer.shape[0]
    chunk = tokens // CHUNKS
    rows = value_weight.shape[0]
    share = rows // n_rep
    width = acc.shape[2]
    per_role = n_rep // 2
    low = mid.shape[1]

    def fs_at(d):
        return lax.rem(f + d, n_fs)

    def rep_at(d):
        return lax.rem(r + d, n_rep)

    def send(src, dst, s, v, **where):
        return pltpu.make_async_remote_copy(
            src_ref=src, dst_ref=dst, send_sem=s, recv_sem=v,
            device_id=where, device_id_type=pl.DeviceIdType.MESH,
        )

    w_loads = [pltpu.make_async_copy(weights[k], w_buf.at[k], w_sem.at[k]) for k in range(2)]
    b_loads = [pltpu.make_async_copy(bases[k], basis_buf.at[k], b_sem.at[k]) for k in range(2)]

    def x_loads(c):
        span = pl.ds(pl.multiple_of(c * chunk, chunk), chunk)
        return [pltpu.make_async_copy(mixer.at[span], x_buf.at[c], x_sem.at[c, 0])] + [
            pltpu.make_async_copy(cots[k].at[span], cot_buf.at[k, c], x_sem.at[c, 1 + k]) for k in range(2)
        ]

    m_loads = [
        pltpu.make_async_copy(ref, moments.at[i], m_sem.at[i])
        for i, ref in enumerate((value_first_hbm, gate_first_hbm, value_second_hbm, gate_second_hbm))
    ]
    for copy in w_loads + b_loads:
        copy.start()
    for c in range(CHUNKS):
        for copy in x_loads(c):
            copy.start()

    for copy in m_loads:
        copy.start()

    barrier = pltpu.get_barrier_semaphore()
    for d in range(1, n_fs):
        pl.semaphore_signal(barrier, inc=1, device_id={"fs": fs_at(d)}, device_id_type=pl.DeviceIdType.MESH)
    for d in range(1, n_rep):
        pl.semaphore_signal(barrier, inc=1, device_id={"rep": rep_at(d)}, device_id_type=pl.DeviceIdType.MESH)
    for d in range(1, n_tp):
        pl.semaphore_signal(
            barrier, inc=1, device_id={"tp": lax.rem(t + d, n_tp)}, device_id_type=pl.DeviceIdType.MESH
        )
    for k in range(2):
        w_loads[k].wait()
        w_half[k] = w_buf[k].astype(BF16)
    pl.semaphore_wait(barrier, n_fs + n_rep + n_tp - 3)

    def share_of(block, part_index):
        return pl.ds(pl.multiple_of(block * rows + part_index * share, share), share)

    w1 = {}
    for d in range(1, n_fs):
        for k in range(2):
            w1[d, k] = send(
                w_half.at[k, pl.ds(pl.multiple_of(r * share, share), share)],
                gathered[k].at[share_of(f, r)],
                w1_send.at[d - 1, k], w1_recv.at[d - 1, k], fs=fs_at(d),
            )
            w1[d, k].start()
    own = []
    for k in range(2):
        copy = pltpu.make_async_copy(
            w_half.at[k], gathered[k].at[pl.ds(pl.multiple_of(f * rows, rows), rows)], own_sem.at[k]
        )
        copy.start()
        own.append(copy)

    for copy in b_loads:
        copy.wait()
    acc[...] = jnp.zeros_like(acc)

    def one_chunk(c, carry):
        for copy in x_loads(c):
            copy.wait()
        x = x_buf[c]
        for k in range(2):
            upper, lower = split(dot(x, basis_buf[k]))
            for q in range(per_role):
                cols = slice(q * width, (q + 1) * width)
                cot = cot_buf[k, c, :, cols]
                acc[k * per_role + q] += dot_first(upper, cot) + dot_first(lower, cot)
        return carry

    lax.fori_loop(0, CHUNKS, one_chunk, 0)
    s1 = {}
    for d in range(1, n_rep):
        s1[d] = send(
            acc.at[rep_at(d)], part_in.at[d - 1], s1_send.at[d - 1], s1_recv.at[d - 1], rep=rep_at(d)
        )
        s1[d].start()

    w2, heard = {}, set()
    near, far = (r + 1 - 2 * lax.rem(r, 2), lax.rem(r + 2, n_rep)) if n_rep == 4 else (None, None)

    def pass_on(d, e, k, owner, peer):
        source = lax.rem(f - d + n_fs, n_fs)
        rows_ref = gathered[k].at[share_of(source, owner)]
        w2[d, e, k] = send(
            rows_ref, rows_ref, w2_send.at[d - 1, e, k], w2_recv.at[d - 1, e, k], rep=peer
        )
        w2[d, e, k].start()

    def forward(d):
        for k in range(2):
            w1[d, k].wait_recv()
            peers = (near, far) if n_rep == 4 else [rep_at(e) for e in range(1, n_rep)]
            for e, peer in enumerate(peers):
                pass_on(d, e, k, r, peer)

    def relay(d):
        if n_rep == 4:
            for e, k, owner, peer in ((0, 0, near, far), (1, 1, far, near)):
                w2[d, e, k].wait_recv()
                heard.add((d, e, k))
                pass_on(d, 2, k, owner, peer)

    forward(1)
    for k in range(2):
        upper, lower = split(dot_first(basis_buf[k], basis_buf[k]))
        gram[k, 0] = upper
        gram[k, 1] = lower

    for d in range(1, n_rep):
        s1[d].wait_recv()
    total = acc[r]
    for d in range(1, n_rep):
        total += part_in[d - 1]
    mid[...] = total.reshape(mid.shape)
    s2 = {}
    for d in range(1, n_fs):
        s2[d] = send(
            mid.at[fs_at(d)], mid_in.at[d - 1], s2_send.at[d - 1], s2_recv.at[d - 1], fs=fs_at(d)
        )
        s2[d].start()
    for d in range(2, n_fs - 1):
        forward(d)
        relay(d - 1)
    for d in range(1, n_fs):
        s2[d].wait_recv()
    small = mid[f]
    for d in range(1, n_fs):
        small += mid_in[d - 1]
    proj_all[r] = small.astype(BF16)

    cols = pl.ds(pl.multiple_of(lax.rem(r, per_role) * width, width), width)
    is_value = r < per_role
    for copy in m_loads:
        copy.wait()
    first = jnp.where(is_value, moments[0, :, cols], moments[1, :, cols])
    second = jnp.where(is_value, moments[2, :, cols], moments[3, :, cols])
    first_new = 0.9 * first + 0.1 * small
    second_new = 0.95 * second + 0.05 * small * small
    scaled[r, f] = (first_new * lax.rsqrt(second_new)).astype(BF16)
    a4, p4, g4 = {}, {}, {}
    for d in range(1, n_fs):
        a4[d] = send(
            scaled.at[r, f], scaled.at[r, f], a_send.at[d - 1], a_recv.at[d - 1], fs=fs_at(d)
        )
        a4[d].start()
    for d in range(1, n_rep):
        p4[d] = send(proj_all.at[r], proj_all.at[r], p_send.at[d - 1], p_recv.at[d - 1], rep=rep_at(d))
        p4[d].start()
    if n_fs > 2:
        forward(n_fs - 1)
        relay(n_fs - 2)
    for d in range(1, n_fs):
        a4[d].wait_recv()
    for d in range(1, n_rep):
        g4[d] = send(scaled.at[r], scaled.at[r], g_send.at[d - 1], g_recv.at[d - 1], rep=rep_at(d))
        g4[d].start()
    relay(n_fs - 1)
    for d in range(1, n_rep):
        g4[d].wait_recv()

    for k in range(2):
        squares = 0.0
        for q in range(per_role):
            s = scaled[k * per_role + q].reshape(n_fs * low, width)
            squares += jnp.sum((dot(gram[k, 0], s) + dot(gram[k, 1], s)) * s.astype(F32))
        sq_buf[0, k] = jnp.full(sq_buf.shape[2:], squares, F32)
    q4 = []
    for d in range(1, n_tp):
        copy = send(
            sq_buf.at[0], sq_buf.at[d], q_send.at[d - 1], q_recv.at[d - 1], tp=lax.rem(t + d, n_tp)
        )
        copy.start()
        q4.append(copy)
    for d in range(1, n_rep):
        p4[d].wait_recv()
    scaled_out[...] = scaled[...].reshape(scaled_out.shape)
    projected_out[...] = proj_all[...]
    for copy in q4:
        copy.wait_recv()
    sums = sq_buf[0]
    for d in range(1, n_tp):
        sums += sq_buf[d]
    squares_out[...] = sums

    for copy in list(w1.values()) + list(s1.values()) + list(s2.values()) + list(a4.values()):
        copy.wait_send()
    for copy in list(p4.values()) + list(g4.values()) + q4:
        copy.wait_send()
    for copy in own:
        copy.wait()
    for key, copy in w2.items():
        copy.wait_send()
        if key not in heard:
            copy.wait_recv()


def finish(
    own_blocks, entries,
    where, value_rows, gate_rows, value_basis, gate_basis, value_weight, gate_weight,
    scaled, projected, squares, value_first, gate_first, value_second, gate_second,
    value_new, gate_new, value_copy, gate_copy, value_step, gate_step,
    value_first_new, gate_first_new, value_second_new, gate_second_new,
):
    step = pl.program_id(0)
    width = scaled.shape[2]
    per_role = scaled.shape[0] // 2
    roles = (
        (value_rows, value_basis, value_weight, value_new, value_copy, value_step),
        (gate_rows, gate_basis, gate_weight, gate_new, gate_copy, gate_step),
    )
    for k, (rows, basis, weight, new, copy, step_out) in enumerate(roles):
        factor = lax.rsqrt(squares[k, :1, :1] / entries + 1e-06)
        for q in range(per_role):
            cols = slice(q * width, (q + 1) * width)
            direction = dot(basis[...], scaled[k * per_role + q]) * factor
            copy[:, cols] = (rows[:, cols].astype(F32) - learn_rate * direction).astype(BF16)

            @pl.when(step < own_blocks)
            def _():
                step_out[:, cols] = direction
                new[:, cols] = weight[:, cols] - learn_rate * direction

    @pl.when(step == 0)
    def _():
        moments = (
            (value_first, value_second, value_first_new, value_second_new),
            (gate_first, gate_second, gate_first_new, gate_second_new),
        )
        for k, (first, second, first_new, second_new) in enumerate(moments):
            for q in range(per_role):
                cols = slice(q * width, (q + 1) * width)
                small = projected[k * per_role + q].astype(F32)
                first_new[:, cols] = 0.9 * first[:, cols] + 0.1 * small
                second_new[:, cols] = 0.95 * second[:, cols] + 0.05 * small * small


def local(sizes, *args):
    n_fs, n_rep, n_tp = sizes
    (mixer, value_cot, gate_cot, value_weight, gate_weight, value_basis, gate_basis,
     value_first, gate_first, value_second, gate_second) = args
    tokens, model = mixer.shape
    half = value_cot.shape[1]
    rows = value_weight.shape[0]
    rank = value_basis.shape[1]
    low = value_first.shape[0]
    width = 2 * half // n_rep
    chunk = tokens // CHUNKS
    any_spec = pl.BlockSpec(memory_space=pl.ANY)
    vmem = pl.BlockSpec(memory_space=pltpu.VMEM)
    dma = pltpu.SemaphoreType.DMA
    scratch = [
        pltpu.VMEM((CHUNKS, chunk, model), BF16),
        pltpu.VMEM((2, CHUNKS, chunk, half), BF16),
        pltpu.VMEM((2, rows, half), F32),
        pltpu.VMEM((2, rows, half), BF16),
        pltpu.VMEM((2, model, rank), BF16),
        pltpu.VMEM((2, 2, rank, rank), BF16),
        pltpu.VMEM((n_rep, rank, width), F32),
        pltpu.VMEM((n_rep - 1, rank, width), F32),
        pltpu.VMEM((n_fs, low, width), F32),
        pltpu.VMEM((n_fs - 1, low, width), F32),
        pltpu.VMEM((n_rep, low, width), BF16),
        pltpu.VMEM((n_rep, n_fs, low, width), BF16),
        pltpu.VMEM((n_tp, 2, 8, 128), F32),
        pltpu.VMEM((4, low, half), F32),
        dma((CHUNKS, 3)), dma((2,)), dma((2,)), dma((2,)), dma((4,)),
        dma((n_fs - 1, 2)), dma((n_fs - 1, 2)),
        dma((n_fs - 1, n_rep - 1, 2)), dma((n_fs - 1, n_rep - 1, 2)),
    ]
    for count in (n_rep, n_fs, n_rep, n_fs, n_rep, n_tp):
        scratch += [dma((count - 1,)), dma((count - 1,))]
    value_rows, gate_rows, scaled, projected, squares = pl.pallas_call(
        functools.partial(exchange, n_fs, n_rep, n_tp),
        out_shape=(
            jax.ShapeDtypeStruct((rows * n_fs, half), BF16),
            jax.ShapeDtypeStruct((rows * n_fs, half), BF16),
            jax.ShapeDtypeStruct((n_rep, rank, width), BF16),
            jax.ShapeDtypeStruct((n_rep, low, width), BF16),
            jax.ShapeDtypeStruct((2, 8, 128), F32),
        ),
        in_specs=[any_spec] * 11,
        out_specs=(any_spec, any_spec, vmem, vmem, vmem),
        scratch_shapes=scratch,
        compiler_params=pltpu.CompilerParams(
            collective_id=0, has_side_effects=True, vmem_limit_bytes=52 * 1024 * 1024
        ),
        name="exchange",
    )(*args)

    block = min(rows, 256)
    own_blocks = rows // block
    blocks = model // block
    where = (lax.axis_index("fs") * own_blocks).astype(jnp.int32).reshape(1)

    def turned(i, w):
        return (lax.rem(w[0] + i, blocks), 0)

    def own(i, w):
        return (jnp.minimum(i, own_blocks - 1), 0)

    def whole(shape):
        return pl.BlockSpec(shape, lambda i, w: (0,) * len(shape))

    row_spec = pl.BlockSpec((block, half), turned)
    basis_spec = pl.BlockSpec((block, rank), turned)
    own_spec = pl.BlockSpec((block, half), own)
    moment = whole((low, half))
    return pl.pallas_call(
        functools.partial(finish, own_blocks, float(model) * half * n_tp),
        grid_spec=pltpu.PrefetchScalarGridSpec(
            num_scalar_prefetch=1,
            grid=(blocks,),
            in_specs=[row_spec, row_spec, basis_spec, basis_spec, own_spec, own_spec,
                      whole(scaled.shape), whole(projected.shape), whole(squares.shape)] + [moment] * 4,
            out_specs=[own_spec, own_spec, row_spec, row_spec, own_spec, own_spec] + [moment] * 4,
        ),
        out_shape=[
            jax.ShapeDtypeStruct((rows, half), F32),
            jax.ShapeDtypeStruct((rows, half), F32),
            jax.ShapeDtypeStruct((model, half), BF16),
            jax.ShapeDtypeStruct((model, half), BF16),
            jax.ShapeDtypeStruct((rows, half), F32),
            jax.ShapeDtypeStruct((rows, half), F32),
        ] + [jax.ShapeDtypeStruct((low, half), F32)] * 4,
        compiler_params=pltpu.CompilerParams(vmem_limit_bytes=40 * 1024 * 1024),
        name="finish",
    )(where, value_rows, gate_rows, value_basis, gate_basis, value_weight, gate_weight,
      scaled, projected, squares, value_first, gate_first, value_second, gate_second)


PIECES = 8
EXTRA = (0, 1, 2, 3, 4)
RELAY_X = ((5, 6), (5,), (5, 6))
RELAY_Y = ((7,), (6, 7), (7,))
EARLY = (
    (0, "open"), (2, "first", 0), (3, "first", 1), (4, "inner", 1), (4, "first", 2), (6, "first", 3),
    (6, "first", 4), (6, "inner", 4), (7, "begin", 0, 0), (9, "begin", 0, 1), (9, "first", 5),
    (9, "inner", 5), (9, "first", 6), (13, "begin", 1, 0), (13, "halve", 0), (13, "inner", 9),
    (14, "relay", 1, 6), (14, "begin", 1, 1), (14, "inner", 2), (14, "inner", 7), (15, "inner", 0),
    (15, "halve", 1), (15, "second", 2), (15, "inner", 12), (15, "first", 7), (15, "inner", 3),
    (15, "inner", 8), (15, "second", 7), (15, "inner", 6), (15, "third", 2), (15, "second", 0),
    (15, "quarter", 0), (15, "gram"), (15, "second", 5), (15, "third", 7), (15, "second", 6),
    (15, "inner", 10), (15, "third", 0), (15, "second", 1),
)
LATE = (
    ("relay", 1, 5), ("quarter", 1), ("second", 4), ("update", 0), ("first", 10), ("third", 5), ("third", 6),
    ("relay", 3, 7), ("third", 1), ("first", 8), ("update", 1), ("second", 3), ("third", 4), ("collect", 0),
    ("collect", 1), ("first", 9), ("first", 12), ("inner", 11), ("second", 10), ("relay", 3, 6), ("again", 0),
    ("first", 11), ("second", 9), ("relay", 2, 6), ("third", 3), ("relay", 3, 5), ("second", 11),
    ("relay", 2, 5), ("again", 1), ("relay", 1, 7), ("third", 10), ("third", 11), ("second", 12),
    ("relay", 2, 7), ("second", 8), ("third", 9), ("third", 8), ("measure", 1), ("third", 12), ("measure", 0),
)


def exchange_block(
    mixer, value_cot, gate_cot, value_weight, gate_weight, value_basis, gate_basis,
    value_first, gate_first, value_second, gate_second,
    gathered, scaled, proj, squares_out, basis, weight, moments,
    x_buf, cot_buf, gram, turned, acc, first_in, second_out, second_in, part, part_in, sq_buf,
    x_sem, c_sem, b_sem, w_sem, m_sem,
    z_send, z_recv, x_send, x_recv, y_send, y_recv, rx_send, rx_recv, ry_send, ry_recv,
    s1_send, s1_recv, s2_send, s2_recv, s3_send, s3_recv, a_send, a_recv,
    g_send, g_recv, p_send, p_recv, q_send, q_recv,
):
    f, r, t = lax.axis_index("fs"), lax.axis_index("rep"), lax.axis_index("tp")
    n_fs = 4
    cots = (value_cot, gate_cot)
    weights = (value_weight, gate_weight)
    bases = (value_basis, gate_basis)
    tokens = mixer.shape[0]
    chunk = tokens // CHUNKS
    rows = value_weight.shape[0]
    share = rows // 4
    piece_rows = 2 * share // PIECES
    low = moments.shape[1]
    width = acc.shape[3]
    ends = jnp.logical_or(f == 0, f == n_fs - 1)
    inner = jnp.logical_not(ends)
    turn = 1 - 2 * (f // 2)
    ahead = f + turn
    behind = jnp.clip(f - turn, 0, n_fs - 1)
    x_at, y_at = lax.rem(r, 2), r // 2
    x_peer, y_peer = r + 1 - 2 * x_at, r + 2 - 4 * y_at
    across = 3 - r
    half_at, part_at = (x_at, y_at), (y_at, x_at)
    half_peer, part_peer = (x_peer, y_peer), (y_peer, x_peer)
    mine = [2 * half_at[k] + part_at[k] for k in range(2)]

    def fs_at(d):
        return lax.rem(f + d, n_fs)

    def send(src, dst, s, v, **where):
        return pltpu.make_async_remote_copy(
            src_ref=src, dst_ref=dst, send_sem=s, recv_sem=v,
            device_id=where, device_id_type=pl.DeviceIdType.MESH,
        )

    def span(start, size):
        return pl.ds(pl.multiple_of(start, size), size)

    def piece(plane, quarter, c):
        return gathered.at[c % 2, span(plane * rows + quarter * share + (c // 2) * piece_rows, piece_rows)]

    z_pieces = [(r, c) for c in range(PIECES)] + [(across, c) for c in EXTRA]
    count = len(z_pieces)
    order = (r, across, x_peer, y_peer)

    def w_load(o, k):
        where = span(order[o] * share, share)
        return pltpu.make_async_copy(weights[k].at[where], weight.at[k, where], w_sem.at[o, k])

    def b_load(k):
        return pltpu.make_async_copy(bases[k], basis.at[k], b_sem.at[k])

    def x_load(c):
        return pltpu.make_async_copy(mixer.at[span(c * chunk, chunk)], x_buf.at[c], x_sem.at[c])

    def c_load(k):
        return pltpu.make_async_copy(cots[k], cot_buf.at[k], c_sem.at[k])

    m_loads = [
        pltpu.make_async_copy(ref, moments.at[i], m_sem.at[i])
        for i, ref in enumerate((value_first, gate_first, value_second, gate_second))
    ]
    b_load(0).start()
    x_load(0).start()
    for o in range(2 if EXTRA else 1):
        for k in range(2):
            w_load(o, k).start()
    for c in range(1, CHUNKS):
        x_load(c).start()
    c_load(0).start()
    b_load(1).start()
    c_load(1).start()
    for copy in m_loads:
        copy.start()
    for o in range(2 if EXTRA else 1, 4):
        for k in range(2):
            w_load(o, k).start()

    barrier = pltpu.get_barrier_semaphore()
    for d in range(1, n_fs):
        pl.semaphore_signal(barrier, inc=1, device_id={"fs": fs_at(d)}, device_id_type=pl.DeviceIdType.MESH)
    for peer in (x_peer, y_peer):
        pl.semaphore_signal(barrier, inc=1, device_id={"rep": peer}, device_id_type=pl.DeviceIdType.MESH)
    pl.semaphore_signal(barrier, inc=1, device_id={"tp": 1 - t}, device_id_type=pl.DeviceIdType.MESH)

    def plane_of(slot):
        return lax.rem(f + turn * slot + n_fs, n_fs)

    landing = jnp.where(ends, 2, 0)

    def own_ahead(i):
        quarter, c = z_pieces[i]
        ref = piece(f, quarter, c)
        return send(ref, ref, z_send.at[0, i], z_recv.at[landing, i], fs=ahead)

    def own_behind(i):
        quarter, c = z_pieces[i]
        ref = piece(f, quarter, c)
        return send(ref, ref, z_send.at[1, i], z_recv.at[0, i], fs=behind)

    def pass_along(slot, i):
        quarter, c = z_pieces[i]
        ref = piece(plane_of(slot), quarter, c)
        if slot == 3:
            return send(ref, ref, z_send.at[4, i], z_recv.at[1, i], fs=ahead)
        return send(ref, ref, z_send.at[1 + slot, i], z_recv.at[slot, i], fs=behind)

    def arrival(slot, i):
        quarter, c = z_pieces[i]
        ref = piece(plane_of(slot), quarter, c)
        return send(ref, ref, z_send.at[0, i], z_recv.at[slot - 1, i], fs=ahead)

    def opening():
        for o in range(2 if EXTRA else 1):
            where = span(order[o] * share, share)
            for k in range(2):
                w_load(o, k).wait()
                gathered[k, span(f * rows + order[o] * share, share)] = weight[k, where].astype(BF16)
        pl.semaphore_wait(barrier, n_fs + 2)
        for i in range(count):
            own_ahead(i).start()

            @pl.when(inner)
            def _():
                own_behind(i).start()

    def to_x(slot, c):
        ref = piece(plane_of(slot), r, c)
        return send(ref, ref, x_send.at[slot - 1, c], x_recv.at[slot - 1, c], rep=x_peer)

    def to_y(slot, c):
        ref = piece(plane_of(slot), r, c)
        return send(ref, ref, y_send.at[slot - 1, c], y_recv.at[slot - 1, c], rep=y_peer)

    def relay_x(slot, c):
        ref = piece(plane_of(slot), y_peer, c)
        return send(ref, ref, rx_send.at[slot - 1, c], rx_recv.at[slot - 1, c], rep=x_peer)

    def relay_y(slot, c):
        ref = piece(plane_of(slot), x_peer, c)
        return send(ref, ref, ry_send.at[slot - 1, c], ry_recv.at[slot - 1, c], rep=y_peer)

    def spread(slot, i):
        if i < PIECES:
            to_x(slot, i).start()
            to_y(slot, i).start()

    def arrive_first(i):
        arrival(1, i).wait_recv()

        @pl.when(inner)
        def _():
            pass_along(1, i).start()

        spread(1, i)

    def arrive_inner(i):
        @pl.when(inner)
        def _():
            arrival(3, i).wait_recv()
            pass_along(3, i).start()

    def arrive_second(i):
        arrival(2, i).wait_recv()

        @pl.when(inner)
        def _():
            pass_along(2, i).start()

        spread(2, i)

    def arrive_third(i):
        @pl.when(ends)
        def _():
            arrival(3, i).wait_recv()

        spread(3, i)

    def relay(slot, c):
        if c in RELAY_X[slot - 1]:
            to_y(slot, c).wait_recv()
            relay_x(slot, c).start()
        if c in RELAY_Y[slot - 1]:
            to_x(slot, c).wait_recv()
            relay_y(slot, c).start()

    def s1(k, j):
        other = acc.at[k, 2 * (1 - half_at[k]) + (part_at[k] if j else 1 - part_at[k])]
        return send(other, first_in.at[k, j], s1_send.at[k, j], s1_recv.at[k, j], rep=half_peer[k])

    def s2(k):
        return send(second_out.at[k], second_in.at[k], s2_send.at[k], s2_recv.at[k], rep=part_peer[k])

    def s3(k, d):
        return send(
            part.at[k, span(fs_at(d) * low, low)], part_in.at[k, d - 1],
            s3_send.at[k, d - 1], s3_recv.at[k, d - 1], fs=fs_at(d),
        )

    def halve(k):
        s1(k, 0).wait_recv()
        second_out[k] = acc[k, 2 * half_at[k] + 1 - part_at[k]] + first_in[k, 0]
        s2(k).start()

    def quarter(k):
        s1(k, 1).wait_recv()
        s2(k).wait_recv()
        part[k] = acc[k, mine[k]] + first_in[k, 1] + second_in[k]
        for d in range(1, n_fs):
            s3(k, d).start()

    def a4(k, d):
        ref = scaled.at[k, mine[k], span(f * low, low)]
        return send(ref, ref, a_send.at[k, d - 1], a_recv.at[k, d - 1], fs=fs_at(d))

    def grow(buf, ss, vs, k, stage):
        if stage == 0:
            ref = buf.at[k, mine[k]]
            return send(ref, ref, ss.at[k, 0], vs.at[k, 0], rep=part_peer[k])
        if stage == 1:
            ref = buf.at[k, mine[k]]
            return send(ref, ref, ss.at[k, 1], vs.at[k, 1], rep=half_peer[k])
        ref = buf.at[k, 2 * half_at[k] + 1 - part_at[k]]
        return send(ref, ref, ss.at[k, 2], vs.at[k, 2], rep=half_peer[k])

    def g4(k, stage):
        return grow(scaled, g_send, g_recv, k, stage)

    def p4(k, stage):
        return grow(proj, p_send, p_recv, k, stage)

    def update(k):
        if k == 0:
            for copy in m_loads:
                copy.wait()
        for d in range(1, n_fs):
            s3(k, d).wait_recv()
        small = part[k, span(f * low, low)]
        for d in range(1, n_fs):
            small += part_in[k, d - 1]
        proj[k, mine[k]] = small.astype(BF16)
        cols = span(mine[k] * width, width)
        first_new = 0.9 * moments[k, :, cols] + 0.1 * small
        second_new = 0.95 * moments[2 + k, :, cols] + 0.05 * small * small
        scaled[k, mine[k], span(f * low, low)] = (first_new * lax.rsqrt(second_new)).astype(BF16)
        for d in range(1, n_fs):
            a4(k, d).start()

    def collect(k):
        for d in range(1, n_fs):
            a4(k, d).wait_recv()
        g4(k, 0).start()
        g4(k, 1).start()
        p4(k, 0).start()
        p4(k, 1).start()

    def collect_second(k):
        g4(k, 0).wait_recv()
        g4(k, 2).start()
        p4(k, 0).wait_recv()
        p4(k, 2).start()

    measured = []
    q4 = send(sq_buf.at[0], sq_buf.at[1], q_send, q_recv, tp=1 - t)

    def measure(k):
        for stage in (1, 2):
            g4(k, stage).wait_recv()
        squares = 0.0
        for n in range(4):
            s = scaled[k, n]
            squares += jnp.sum((dot(gram[k, 0], s) + dot(gram[k, 1], s)) * s.astype(F32))
        sq_buf[0, k] = jnp.full(sq_buf.shape[2:], squares, F32)
        measured.append(k)
        if len(measured) == 2:
            q4.start()

    def make_gram():
        for k in range(2):
            upper, lower = split(dot_first(basis[k], basis[k]))
            gram[k, 0] = upper
            gram[k, 1] = lower

    jobs = {
        "open": opening, "begin": lambda k, j: s1(k, j).start(), "first": arrive_first, "inner": arrive_inner,
        "second": arrive_second, "third": arrive_third, "relay": relay, "halve": halve,
        "quarter": quarter, "update": update, "collect": collect, "again": collect_second,
        "measure": measure, "gram": make_gram,
    }
    rank = basis.shape[2]

    def one_step(i, carry):
        k, at = i // (CHUNKS + 4), lax.rem(i, CHUNKS + 4)
        for first in sorted({entry[0] for entry in EARLY}):
            @pl.when(i == first)
            def _():
                for entry in EARLY:
                    if entry[0] == first:
                        jobs[entry[1]](*entry[2:])

        for role in range(2):
            @pl.when(i == role * (CHUNKS + 4))
            def _():
                b_load(role).wait()

            @pl.when(i == role * (CHUNKS + 4) + CHUNKS)
            def _():
                c_load(role).wait()

        @pl.when(i < CHUNKS)
        def _():
            x_load(at).wait()

        @pl.when(at < CHUNKS)
        def _():
            upper, lower = split(
                lax.dot_general(basis[k], x_buf[at], (((0,), (1,)), ((), ())), preferred_element_type=F32)
            )
            turned[:rank, span(at * chunk, chunk)] = upper
            turned[rank:, span(at * chunk, chunk)] = lower

        @pl.when(at >= CHUNKS)
        def _():
            j = at - CHUNKS
            half_on, part_on = jnp.where(k == 0, x_at, y_at), jnp.where(k == 0, y_at, x_at)
            half_now = jnp.where(j < 2, 1 - half_on, half_on)
            part_now = jnp.where(lax.rem(j, 2) == 0, 1 - part_on, part_on)
            n = 2 * half_now + part_now
            cot = cot_buf[k, :, span(n * width, width)]
            acc[k, n] = dot(turned[:rank], cot) + dot(turned[rank:], cot)

        return carry

    lax.fori_loop(0, 2 * (CHUNKS + 4), one_step, 0)
    for name, *where in LATE:
        jobs[name](*where)

    for k in range(2):
        for stage in (1, 2):
            p4(k, stage).wait_recv()
    for slot in (1, 2, 3):
        for c in range(PIECES):
            if c not in RELAY_X[slot - 1]:
                to_y(slot, c).wait_recv()
            else:
                relay_x(slot, c).wait_recv()
                relay_x(slot, c).wait_send()
            if c not in RELAY_Y[slot - 1]:
                to_x(slot, c).wait_recv()
            else:
                relay_y(slot, c).wait_recv()
                relay_y(slot, c).wait_send()
            to_x(slot, c).wait_send()
            to_y(slot, c).wait_send()
    for i in range(count):
        own_ahead(i).wait_send()

        @pl.when(inner)
        def _():
            own_behind(i).wait_send()
            for slot in (1, 2, 3):
                pass_along(slot, i).wait_send()
    for k in range(2):
        s1(k, 0).wait_send()
        s1(k, 1).wait_send()
        s2(k).wait_send()
        for d in range(1, n_fs):
            s3(k, d).wait_send()
            a4(k, d).wait_send()
        for stage in range(3):
            g4(k, stage).wait_send()
            p4(k, stage).wait_send()
    for o in range(2 if EXTRA else 1, 4):
        for k in range(2):
            w_load(o, k).wait()
    q4.wait()
    squares_out[...] = sq_buf[0] + sq_buf[1]


def finish_block(
    entries, gathered, scaled, proj, squares, basis, weight, moments,
    value_new, gate_new, value_copy, gate_copy, value_step, gate_step,
    value_first_new, gate_first_new, value_second_new, gate_second_new,
    new_buf, step_buf, copy_buf, moment_buf, new_sem, step_sem, copy_sem, moment_sem,
):
    f = lax.axis_index("fs")
    rows = weight.shape[1]
    model = gathered.shape[1]
    width = scaled.shape[3]
    block = min(rows, 256)
    own = rows // block
    blocks = model // block
    news, copies, steps = (value_new, gate_new), (value_copy, gate_copy), (value_step, gate_step)
    factors = [lax.rsqrt(squares[k, :1, :1] / entries + 1e-06) for k in range(2)]

    def span(start, size):
        return pl.ds(pl.multiple_of(start, size), size)

    def row_of(b):
        return lax.rem(f * own + b, blocks) * block

    def new_out(k, b):
        return pltpu.make_async_copy(
            new_buf.at[k, span(b * block, block)], news[k].at[span(b * block, block)], new_sem.at[k, b])

    def step_store(k, b):
        return pltpu.make_async_copy(
            step_buf.at[k, span(b * block, block)], steps[k].at[span(b * block, block)], step_sem.at[k, b])

    def copy_out(k, b):
        where = span(row_of(b), block)
        return pltpu.make_async_copy(copy_buf.at[k, where], copies[k].at[where], copy_sem.at[k, b])

    def own_block(b, carry):
        for k in range(2):
            where = span(row_of(b), block)
            local_rows = span(b * block, block)
            for n in range(4):
                cols = slice(n * width, (n + 1) * width)
                direction = dot(basis[k, where], scaled[k, n]) * factors[k]
                updated = weight[k, local_rows, cols] - learn_rate * direction
                step_buf[k, local_rows, cols] = direction
                new_buf[k, local_rows, cols] = updated
                copy_buf[k, where, cols] = updated.astype(BF16)
            step_store(k, b).start()
            new_out(k, b).start()
            copy_out(k, b).start()
        return carry

    lax.fori_loop(0, own, own_block, 0)
    outs = (value_first_new, gate_first_new, value_second_new, gate_second_new)
    for k in range(2):
        for n in range(4):
            cols = slice(n * width, (n + 1) * width)
            small = proj[k, n].astype(F32)
            moment_buf[k, :, cols] = 0.9 * moments[k, :, cols] + 0.1 * small
            moment_buf[2 + k, :, cols] = 0.95 * moments[2 + k, :, cols] + 0.05 * small * small
    moment_outs = [pltpu.make_async_copy(moment_buf.at[i], outs[i], moment_sem.at[i]) for i in range(4)]
    for copy in moment_outs:
        copy.start()

    def other_block(b, carry):
        for k in range(2):
            where = span(row_of(b), block)
            for n in range(4):
                cols = slice(n * width, (n + 1) * width)
                direction = dot(basis[k, where], scaled[k, n]) * (learn_rate * factors[k])
                copy_buf[k, where, cols] = (gathered[k, where, cols].astype(F32) - direction).astype(BF16)
            copy_out(k, b).start()
        return carry

    lax.fori_loop(own, blocks, other_block, 0)

    def drain_own(b, carry):
        for k in range(2):
            step_store(k, b).wait()
            new_out(k, b).wait()
        return carry

    def drain(b, carry):
        for k in range(2):
            copy_out(k, b).wait()
        return carry

    lax.fori_loop(0, own, drain_own, 0)
    lax.fori_loop(0, blocks, drain, 0)
    for copy in moment_outs:
        copy.wait()


def local_block(*args):
    (mixer, value_cot, gate_cot, value_weight, gate_weight, value_basis, gate_basis,
     value_first, gate_first, value_second, gate_second) = args
    n_fs = 4
    tokens, model = mixer.shape
    half = value_cot.shape[1]
    rows = value_weight.shape[0]
    rank = value_basis.shape[1]
    low = value_first.shape[0]
    width = half // 4
    chunk = tokens // CHUNKS
    count = PIECES + len(EXTRA)
    hbm = pl.BlockSpec(memory_space=pltpu.HBM)
    vmem = pl.BlockSpec(memory_space=pltpu.VMEM)
    dma = pltpu.SemaphoreType.DMA
    scratch = [
        pltpu.VMEM((CHUNKS, chunk, model), BF16),
        pltpu.VMEM((2, tokens, half), BF16),
        pltpu.VMEM((2, 2, rank, rank), BF16),
        pltpu.VMEM((2 * rank, tokens), BF16),
        pltpu.VMEM((2, 4, rank, width), F32),
        pltpu.VMEM((2, 2, rank, width), F32),
        pltpu.VMEM((2, rank, width), F32),
        pltpu.VMEM((2, rank, width), F32),
        pltpu.VMEM((2, rank, width), F32),
        pltpu.VMEM((2, n_fs - 1, low, width), F32),
        pltpu.VMEM((2, 2, 8, 128), F32),
        dma((CHUNKS,)), dma((2,)), dma((2,)), dma((4, 2)), dma((4,)),
        dma((5, count)), dma((3, count)),
    ]
    scratch += [dma((3, PIECES)) for _ in range(8)]
    scratch += [dma((2, 2)), dma((2, 2)), dma((2,)), dma((2,))]
    scratch += [dma((2, 3)) for _ in range(8)]
    scratch += [dma(()), dma(())]
    outs = pl.pallas_call(
        exchange_block,
        out_shape=(
            pltpu.VMEM((2, model, half), BF16),
            pltpu.VMEM((2, 4, rank, width), BF16),
            pltpu.VMEM((2, 4, low, width), BF16),
            pltpu.VMEM((2, 8, 128), F32),
            pltpu.VMEM((2, model, rank), BF16),
            pltpu.VMEM((2, rows, half), F32),
            pltpu.VMEM((4, low, half), F32),
        ),
        in_specs=[hbm] * 11,
        out_specs=(vmem,) * 7,
        scratch_shapes=scratch,
        compiler_params=pltpu.CompilerParams(
            collective_id=0, has_side_effects=True, vmem_limit_bytes=VMEM_FIRST
        ),
        name="exchange_block",
    )(*args)
    outs = [pltpu.with_memory_space_constraint(out, pltpu.VMEM) for out in outs]
    block = min(rows, 256)
    return pl.pallas_call(
        functools.partial(finish_block, float(model) * half * 2),
        in_specs=[vmem] * 7,
        out_specs=[hbm] * 10,
        out_shape=[
            jax.ShapeDtypeStruct((rows, half), F32),
            jax.ShapeDtypeStruct((rows, half), F32),
            jax.ShapeDtypeStruct((model, half), BF16),
            jax.ShapeDtypeStruct((model, half), BF16),
            jax.ShapeDtypeStruct((rows, half), F32),
            jax.ShapeDtypeStruct((rows, half), F32),
        ] + [jax.ShapeDtypeStruct((low, half), F32)] * 4,
        scratch_shapes=[
            pltpu.VMEM((2, rows, half), F32),
            pltpu.VMEM((2, rows, half), F32),
            pltpu.VMEM((2, model, half), BF16),
            pltpu.VMEM((4, low, half), F32),
            dma((2, rows // block)), dma((2, rows // block)), dma((2, model // block)), dma((4,)),
        ],
        compiler_params=pltpu.CompilerParams(vmem_limit_bytes=VMEM_SECOND),
        name="finish_block",
    )(*outs)


def solution(mesh):
    sizes = tuple(mesh.shape[name] for name in ("fs", "rep", "tp"))
    return jax.shard_map(
        lambda *args: tuple(local_block(*args) if sizes == (4, 4, 2) else local(sizes, *args)),
        mesh=mesh,
        in_specs=(
            P(("fs", "rep"), None),
            P(("fs", "rep"), "tp"),
            P(("fs", "rep"), "tp"),
            P("fs", "tp"),
            P("fs", "tp"),
            P(),
            P(),
            P("fs", "tp"),
            P("fs", "tp"),
            P("fs", "tp"),
            P("fs", "tp"),
        ),
        out_specs=(
            P("fs", "tp"),
            P("fs", "tp"),
            P(None, "tp"),
            P(None, "tp"),
            P("fs", "tp"),
            P("fs", "tp"),
            P("fs", "tp"),
            P("fs", "tp"),
            P("fs", "tp"),
            P("fs", "tp"),
        ),
        check_vma=False,
    )
```
